128 devices in a mesh: grp: 4 (over y, x), ep: 32 (over z, core).
Axes of the slice: x: 2, y: 2, z: 16, core: 2. Of those that a mesh axis runs over, the one named last changes fastest.
The devices are a block of a 8x8x16 slice.
Arguments:
- hidden: bfloat16 [1024, 2048], P(('grp', 'ep')), parts along dimension 0, may hold values from -6 to 6
- norm_gain: bfloat16 [2048], replicated, may hold values from 0.099609375 to 1.8984375
- outgate_weight: bfloat16 [2048, 2048], P(None, 'ep'), may hold values from -0.125 to 0.125
- input_weight: bfloat16 [2048, 2048], P(None, 'ep'), may hold values from -0.125 to 0.125
- write_weight: bfloat16 [2048, 512], P(None, 'ep'), may hold values from -0.125 to 0.125
- read_weight: bfloat16 [2048, 512], P(None, 'ep'), may hold values from -0.125 to 0.125
- step_weight: bfloat16 [2048, 32], replicated, may hold values from -0.125 to 0.125
- step_bias: float32 [32], replicated, may hold values from -1.5 to 1
- decay_log: float32 [32], replicated, may hold values from -3 to 1
- skip_gain: float32 [32], replicated, may hold values from 0.1 to 1.9
- conv_weight: bfloat16 [4, 3072], replicated, may hold values from -3 to 3
- conv_state: bfloat16 [1024, 3, 3072], P(('grp', 'ep')), parts along dimension 0, may hold values from -6 to 6
- mixer_state: float32 [1024, 32, 64, 128], P(('grp', 'ep')), parts along dimension 0, may hold values from -3 to 3
- inner_gain: bfloat16 [2048], replicated, may hold values from 0.099609375 to 1.8984375
- out_weight: bfloat16 [2048, 2048], P('ep'), may hold values from -0.125 to 0.125
- ffn_gain: bfloat16 [2048], replicated, may hold values from 0.099609375 to 1.8984375
- expert_gate: bfloat16 [2048, 28672], P(None, 'ep'), may hold values from -0.125 to 0.125
- expert_up: bfloat16 [2048, 28672], P(None, 'ep'), may hold values from -0.125 to 0.125
- expert_down: bfloat16 [28672, 2048], P('ep'), may hold values from -0.09375 to 0.09375
- route_ids: int32 [1024, 2], P(('grp', 'ep')), parts along dimension 0, may hold values from 0 to 7, all different within a row; in each aligned block of 8 rows (0 to 7, 8 to 15, ...) at most 8 rows name the same one
- route_weights: float32 [1024, 2], P(('grp', 'ep')), parts along dimension 0, may hold values from 0.1 to 1
Outputs:
- result: bfloat16 [1024, 2048], P(('grp', 'ep')), parts along dimension 0
- new_state: float32 [1024, 32, 64, 128], P(('grp', 'ep')), parts along dimension 0
- new_conv: bfloat16 [1024, 3, 3072], P(('grp', 'ep')), parts along dimension 0
The draws below stay inside these ranges and needn't reach their ends.
There are 4 independent parts, one for each index of `grp`. The reference program is written for one: setup_inputs(seed, part) draws one part's arguments, and reference() takes and returns one part's arrays. A program takes and returns all parts, laid end to end along the dimension named above; an argument that names none is the same for every part. Nothing has to cross between parts.
Inputs may be any that keep to these rules, and one draw needn't show every extreme that they name: `route_ids`: each row names 2 different experts; the rows of one device name one expert at most 8 times.
All inputs are finite; a program needn't handle non-finite values.
Results may differ from the reference program's by a relative error of at most 0.02.
Values may be sent and summed in bfloat16 or wider, within the bound.
A program may use at most 128 MiB of HBM per device.

```python
import math
import jax
import jax.numpy as jnp
import numpy as np
from jax import lax

D = 2048
HEADS = 32
HEAD_DIM = 64
GROUPS = 4
STATE = 128
CONV_W = 4
EXPERTS = 8
EXPERT_FF = 3584
TOP = 2
SEQ_DEV = 8
INNER = 2048
CONV_DIM = 3072
SEQS = 256


def level_of(stream_key, shape, shards, least, top_value):
    def one(position, shards_of):
        heights = jax.random.uniform(jax.random.fold_in(jax.random.fold_in(stream_key, 6), position), (shards_of,), jnp.float32, least / len(shards), top_value / len(shards))
        return jnp.repeat(jnp.exp(heights), shape[position] // shards_of).reshape((-1,) + (1,) * (len(shape) - position - 1))

    gain = one(*shards[0])
    for cut in shards[1:]:
        gain = gain * one(*cut)
    return gain


def deal_out(stream_key, own, number, rows, amount, top, reach, slope):
    order = jax.random.permutation(stream_key, amount)
    crowded, common = portions_of(amount, rows * top, reach, slope, True), portions_of(amount, rows * top, reach, slope, False)
    places = jnp.arange(amount)

    def named(sizes, rotation):
        used = int((sizes > 0).sum())
        fixed = max(1, used // 4)
        passed = fixed + (places - fixed + rotation * (used - fixed)) % max(1, amount - fixed)
        return jnp.zeros((amount,), jnp.int32).at[order[jnp.where(places < fixed, places, passed)]].set(jnp.asarray(sizes, jnp.int32))

    sizes = jnp.where(number % 4 == 0, named(crowded, number // 4), named(common, number - number // 4 - 1))
    mixed = jax.random.permutation(jax.random.fold_in(own, 3), amount)
    source_of, taker = mixed[0:amount // 2 * 2:2], mixed[1:amount // 2 * 2:2]
    margin = jnp.minimum(sizes[source_of] - 1, reach - sizes[taker]) // 2
    margin = jnp.where((source_of == order[0]) | (taker == order[0]) | (sizes[taker] == 0), 0, jnp.maximum(margin, 0))
    passed = jax.random.randint(jax.random.fold_in(own, 4), (amount // 2,), 0, 1 << 20) % (margin + 1)
    sizes = sizes.at[source_of].add(-passed).at[taker].add(passed)
    items = jnp.searchsorted(jnp.cumsum(sizes), jnp.arange(rows * top), side="right").astype(jnp.int32)
    table = items.reshape(top, rows).T
    table = table[jax.random.permutation(jax.random.fold_in(own, 1), rows)]
    rotation = jax.random.randint(jax.random.fold_in(own, 2), (rows, 1), 0, top)
    return jnp.take_along_axis(table, (jnp.arange(top)[None, :] + rotation) % top, axis=1)


def portions_of(number_of, total, reach, slope, full):
    loads = [(1 << 20) // math.isqrt(grade ** slope) + 1 for grade in range(1, number_of + 1)]
    largest = reach if full else min(reach, max(-(-total // number_of), total * loads[0] // sum(loads)))
    least = 1 if total - largest >= number_of - 1 else 0
    counts, rest = [largest] + [least] * (number_of - 1), total - largest - least * (number_of - 1)
    while rest > 0:
        free = [i for i in range(1, number_of) if counts[i] < largest] or [i for i in range(1, number_of) if counts[i] < reach]
        whole, remaining = sum([loads[i] for i in free]), rest
        for i in free:
            more = min(reach - counts[i], max(1, remaining * loads[i] // whole), rest)
            counts[i] = counts[i] + more
            rest = rest - more
    return np.array(counts)


def noise(own_key, extent, width, most, pieces=(), held_as=jnp.bfloat16):
    array = jax.random.normal(own_key, extent, jnp.float32) * width
    if len(pieces) > 0:
        array = level_of(own_key, extent, pieces, -0.22, 0.18) * array
    return jnp.clip(array, min=-most, max=most).astype(held_as)


def setup_inputs(seed: int = 0, part: int = 0) -> dict:
    arg_keys = jax.random.split(jax.random.key(seed), 22)
    own_keys = jax.random.split(jax.random.fold_in(arg_keys[21], part), 22)
    hidden = noise(own_keys[0], (SEQS, D), 1.0, 6.0, ((0, 32),))
    norm_gain = jnp.clip(1.0 + 0.18 * jax.random.normal(arg_keys[1], (D,), jnp.float32), 0.099609375, 1.8984375).astype(jnp.bfloat16)
    outgate_weight = noise(arg_keys[2], (D, INNER), D ** -0.5, 0.125, ((1, 32),))
    input_weight = noise(arg_keys[3], (D, INNER), D ** -0.5, 0.125, ((1, 32),))
    write_weight = noise(arg_keys[4], (D, GROUPS * STATE), D ** -0.5, 0.125, ((1, 32),))
    read_weight = noise(arg_keys[5], (D, GROUPS * STATE), D ** -0.5, 0.125, ((1, 32),))
    step_weight = noise(arg_keys[6], (D, HEADS), D ** -0.5, 0.125)
    step_bias = jnp.clip(jax.random.uniform(arg_keys[7], (HEADS,), jnp.float32, -1.5, 1.0), -1.5, 1.0)
    decay_log = jnp.clip(jax.random.uniform(arg_keys[8], (HEADS,), jnp.float32, -3.0, 1.0), -3.0, 1.0)
    skip_gain = jnp.clip(1.0 + 0.18 * jax.random.normal(arg_keys[9], (HEADS,), jnp.float32), 0.1, 1.9)
    conv_weight = noise(arg_keys[10], (CONV_W, CONV_DIM), CONV_W ** -0.5, 3.0)
    conv_state = noise(own_keys[11], (SEQS, CONV_W - 1, CONV_DIM), 1.0, 6.0, ((0, 32),))
    mixer_state = noise(own_keys[12], (SEQS, HEADS, HEAD_DIM, STATE), 0.3, 3.0, ((0, 32),), jnp.float32)
    inner_gain = jnp.clip(1.0 + 0.18 * jax.random.normal(arg_keys[13], (INNER,), jnp.float32), 0.099609375, 1.8984375).astype(jnp.bfloat16)
    out_weight = noise(arg_keys[14], (INNER, D), INNER ** -0.5, 0.125, ((0, 32),))
    ffn_gain = jnp.clip(1.0 + 0.18 * jax.random.normal(arg_keys[15], (D,), jnp.float32), 0.099609375, 1.8984375).astype(jnp.bfloat16)
    expert_gate = noise(arg_keys[16], (D, EXPERTS * EXPERT_FF), D ** -0.5, 0.125, ((1, 32),))
    expert_up = noise(arg_keys[17], (D, EXPERTS * EXPERT_FF), D ** -0.5, 0.125, ((1, 32),))
    expert_down = noise(arg_keys[18], (EXPERTS * EXPERT_FF, D), EXPERT_FF ** -0.5, 0.09375, ((0, 32),))
    route_ids_keys = jax.random.split(jax.random.fold_in(own_keys[19], 1), SEQS // SEQ_DEV)
    route_ids_turns = jax.random.permutation(jax.random.fold_in(own_keys[19], 3), SEQS // SEQ_DEV)
    route_ids = jax.vmap(lambda own, number: deal_out(jax.random.fold_in(own_keys[19], 2), own, number, SEQ_DEV, EXPERTS, TOP, SEQ_DEV, 2))(route_ids_keys, route_ids_turns).reshape((SEQS, TOP))
    route_weights = jnp.clip(0.1 + 0.9 * jax.random.uniform(own_keys[20], (SEQS, TOP), jnp.float32) ** level_of(own_keys[20], (SEQS, TOP), ((0, 32),), -0.2, 0.2), 0.1, 1.0)
    return dict(hidden=hidden, norm_gain=norm_gain, outgate_weight=outgate_weight, input_weight=input_weight, write_weight=write_weight, read_weight=read_weight, step_weight=step_weight, step_bias=step_bias, decay_log=decay_log, skip_gain=skip_gain, conv_weight=conv_weight, conv_state=conv_state, mixer_state=mixer_state, inner_gain=inner_gain, out_weight=out_weight, ffn_gain=ffn_gain, expert_gate=expert_gate, expert_up=expert_up, expert_down=expert_down, route_ids=route_ids, route_weights=route_weights)


norm_eps = 1e-06

def rms_scale(values, gain_vec):
    floats = values.astype(jnp.float32)
    scaled = floats * lax.rsqrt(lax.optimization_barrier(jnp.mean(floats * floats, axis=-1, keepdims=True)) + norm_eps)
    return scaled * gain_vec.astype(jnp.float32)

def mixer_step(gate_proj, input_proj, write_proj, read_proj, step_raw, step_bias, decay_log, skip_gain, conv_weight, conv_state, mixer_state, inner_gain):
    seqs_here, head_count, head_dim, state_width = mixer_state.shape
    group_count = write_proj.shape[1] // state_width
    per_group = head_count // group_count
    inner_width = head_count * head_dim
    new_row = jnp.concatenate([input_proj, write_proj, read_proj], axis=1)
    window = jnp.concatenate([conv_state, new_row[:, None, :]], axis=1)
    conv_out = jax.nn.silu(lax.optimization_barrier(jnp.sum(window.astype(jnp.float32) * conv_weight.astype(jnp.float32)[None], axis=1)))
    conv_inputs = conv_out[:, :inner_width].reshape(seqs_here, group_count, per_group, head_dim)
    split_at = inner_width + group_count * state_width
    write_map = conv_out[:, inner_width:split_at].reshape(seqs_here, group_count, state_width)
    read_map = conv_out[:, split_at:].reshape(seqs_here, group_count, state_width)
    step_size = jax.nn.softplus(step_raw + step_bias)
    decay_rate = jnp.exp(-step_size * jnp.exp(decay_log)).reshape(seqs_here, group_count, per_group)
    scaled_inputs = conv_inputs * step_size.reshape(seqs_here, group_count, per_group)[..., None]
    old_state = mixer_state.reshape(seqs_here, group_count, per_group, head_dim, state_width)
    new_state = decay_rate[..., None, None] * old_state + jnp.einsum('sgrp,sgn->sgrpn', scaled_inputs, write_map, precision=lax.Precision.HIGHEST)
    read_out = jnp.einsum('sgrpn,sgn->sgrp', new_state, read_map, precision=lax.Precision.HIGHEST)
    read_out = read_out + skip_gain.reshape(group_count, per_group)[None, :, :, None] * conv_inputs
    gated_in = read_out.reshape(seqs_here, inner_width) * jax.nn.silu(gate_proj.astype(jnp.float32))
    gated = rms_scale(gated_in, inner_gain).astype(jnp.bfloat16)
    return (gated, new_state.reshape(mixer_state.shape), window[:, 1:])

def reference(hidden, norm_gain, outgate_weight, input_weight, write_weight, read_weight, step_weight, step_bias, decay_log, skip_gain, conv_weight, conv_state, mixer_state, inner_gain, out_weight, ffn_gain, expert_gate, expert_up, expert_down, route_ids, route_weights):
    normed = rms_scale(hidden, norm_gain).astype(jnp.bfloat16)
    gate_proj = jnp.dot(normed, outgate_weight, preferred_element_type=jnp.float32).astype(jnp.bfloat16)
    input_proj = jnp.dot(normed, input_weight, preferred_element_type=jnp.float32).astype(jnp.bfloat16)
    write_proj = jnp.dot(normed, write_weight, preferred_element_type=jnp.float32).astype(jnp.bfloat16)
    read_proj = jnp.dot(normed, read_weight, preferred_element_type=jnp.float32).astype(jnp.bfloat16)
    step_raw = jnp.dot(normed, step_weight, preferred_element_type=jnp.float32)
    gated, new_state, new_conv = mixer_step(gate_proj, input_proj, write_proj, read_proj, step_raw, step_bias, decay_log, skip_gain, conv_weight, conv_state, mixer_state, inner_gain)
    mixed_out = jnp.dot(gated, out_weight, preferred_element_type=jnp.float32)
    residual = (hidden.astype(jnp.float32) + mixed_out).astype(jnp.bfloat16)
    normed_ffn = rms_scale(residual, ffn_gain).astype(jnp.bfloat16)
    expert_width = expert_gate.shape[1] // EXPERTS
    moe_sum = jnp.zeros(hidden.shape, jnp.float32)
    for expert in range(EXPERTS):
        first_col = expert * expert_width
        gate_part = jnp.dot(normed_ffn, expert_gate[:, first_col:first_col + expert_width], preferred_element_type=jnp.float32)
        up_part = jnp.dot(normed_ffn, expert_up[:, first_col:first_col + expert_width], preferred_element_type=jnp.float32)
        units = (jax.nn.silu(gate_part) * up_part).astype(jnp.bfloat16)
        expert_out = jnp.dot(units, expert_down[first_col:first_col + expert_width], preferred_element_type=jnp.float32)
        combine = lax.optimization_barrier(jnp.sum(jnp.where(route_ids == expert, route_weights, jnp.zeros((), jnp.float32)), axis=1))
        moe_sum = moe_sum + combine[:, None] * expert_out
    result = (residual.astype(jnp.float32) + moe_sum).astype(jnp.bfloat16)
    return (result, new_state, new_conv)
```

```python
import functools

import jax
import jax.numpy as jnp
from jax import lax
from jax.experimental import pallas as pl
from jax.experimental.pallas import tpu as pltpu
from jax.sharding import PartitionSpec as P

EXPERTS = 8
GRP_EP = ("grp", "ep")
MESH = pl.DeviceIdType.MESH
F32 = jnp.float32
BF16 = jnp.bfloat16
norm_eps = 1e-06

TREE = (((0, 3), (0, 1)), ((3, 6), (3, 4), (1, 2)), ((6, 8), (6, 7), (4, 5)))
EDGES = tuple(
    (sign, f, t) for phase in TREE for (f, t) in phase for sign in (1, -1) if not (t == 8 and sign < 0)
)
SLOT = {edge: k for k, edge in enumerate(EDGES)}
GREET = (1, -1, 2, -2, 3, -3)


def rms_scale(floats, gain):
    return floats * lax.rsqrt(jnp.mean(floats * floats, axis=-1, keepdims=True) + norm_eps) * gain


def nt_dot(a, b):
    return lax.dot_general(a, b, (((1,), (1,)), ((), ())), preferred_element_type=F32)


def step_kernel(
    chips,
    hidden_ref,
    norm_gain_ref,
    outgate_ref,
    input_ref,
    write_ref,
    read_ref,
    step_weight_ref,
    step_bias_ref,
    decay_log_ref,
    skip_gain_ref,
    conv_weight_ref,
    conv_state_ref,
    mixer_state_ref,
    inner_gain_ref,
    out_weight_ref,
    ffn_gain_ref,
    expert_gate_ref,
    expert_up_ref,
    expert_down_ref,
    ids_ref,
    route_ref,
    result_ref,
    new_state_ref,
    new_conv_ref,
    rows_a,
    rows_e,
    proj_w,
    out_w,
    gate_w,
    up_w,
    down_w,
    proj_send,
    proj_recv,
    head_send,
    head_recv,
    part32,
    part_send,
    part_recv,
    units,
    reps,
    conv_part,
    scaled_ref,
    maps_ref,
    rate_ref,
    weight_sem,
    pair_send,
    pair_recv,
    gather_send,
    gather_recv,
    swap_send,
    swap_recv,
    sum_send,
    sum_recv,
):
    seqs, width = hidden_ref.shape
    heads, head_dim, state_width = mixer_state_ref.shape[1:]
    groups = (conv_weight_ref.shape[1] - width) // (2 * state_width)
    per_group = heads // groups
    group_width = per_group * head_dim
    lanes = width // chips
    half = outgate_ref.shape[0]
    thin = write_ref.shape[0]
    hidden_units = expert_gate_ref.shape[1]
    ep = lax.axis_index("ep")
    chip, core = ep // 2, ep % 2

    def at(offset):
        return lax.rem(chip + offset + chips, chips)

    def dev(where):
        return {"ep": where * 2 + core}

    sibling = {"ep": chip * 2 + 1 - core}

    barrier = pltpu.get_barrier_semaphore()
    for offset in GREET:
        pl.semaphore_signal(barrier, inc=1, device_id=dev(at(offset)), device_id_type=MESH)
    pl.semaphore_signal(barrier, inc=1, device_id=sibling, device_id_type=MESH)

    def own_rows(buf, first, count):
        return buf.at[pl.ds(pl.multiple_of(first + count * core, count), count)]

    def own_cols(buf):
        return buf.at[:, pl.ds(pl.multiple_of(hidden_units * core, 128), hidden_units)]

    shards = (
        (outgate_ref, own_rows(proj_w, 0, half)),
        (input_ref, own_rows(proj_w, 2 * half, half)),
        (write_ref, own_rows(proj_w, 4 * half, thin)),
        (read_ref, own_rows(proj_w, 4 * half + 2 * thin, thin)),
        (out_weight_ref, own_rows(out_w, 0, half)),
        (expert_gate_ref, own_cols(gate_w)),
        (expert_up_ref, own_cols(up_w)),
        (expert_down_ref, own_rows(down_w, 0, hidden_units)),
    )
    local = [pltpu.make_async_copy(src, dst, weight_sem.at[k]) for k, (src, dst) in enumerate(shards)]
    local.append(pltpu.make_async_copy(mixer_state_ref, new_state_ref, weight_sem.at[len(shards)]))
    for k in (0, 1, 2, 3):
        local[k].start()

    hidden = hidden_ref[...].astype(F32)
    normed = rms_scale(hidden, norm_gain_ref[...].astype(F32)).astype(BF16)
    rows_a[chip] = normed
    pl.semaphore_wait(barrier, len(GREET) + 1)

    pair = [
        pltpu.make_async_remote_copy(
            src_ref=src, dst_ref=dst, send_sem=pair_send.at[k], recv_sem=pair_recv.at[k], device_id=sibling, device_id_type=MESH
        )
        for k, (src, dst) in enumerate(shards)
    ]

    def all_gather(buf, n):
        started, seen = [], set()

        def copy(edge, source, where):
            k = SLOT[edge]
            return pltpu.make_async_remote_copy(
                src_ref=buf.at[source],
                dst_ref=buf.at[source],
                send_sem=gather_send.at[n, k],
                recv_sem=gather_recv.at[n, k],
                device_id=dev(where),
                device_id_type=MESH,
            )

        def arrive(sign, offset):
            if offset and (sign, offset) not in seen:
                seen.add((sign, offset))
                (edge,) = [e for e in EDGES if e[0] == sign and e[2] == offset]
                copy(edge, at(-sign * offset), chip).wait_recv()

        for sign, f, t in EDGES:
            arrive(sign, f)
            c = copy((sign, f, t), at(-sign * f), at(sign * (t - f)))
            c.start()
            started.append(c)
            if (sign, f, t) == EDGES[3]:
                yield
        for sign, f, t in EDGES:
            arrive(sign, t)
        for c in started:
            c.wait_send()

    def swap(send, recv, n):
        copies = []
        for k in range(1, chips):
            offset = (k + 1) // 2 * (1 if k % 2 else -1)
            there = at(offset)
            copies.append(
                pltpu.make_async_remote_copy(
                    src_ref=send.at[there],
                    dst_ref=recv.at[chip],
                    send_sem=swap_send.at[n, k],
                    recv_sem=swap_recv.at[n, chip],
                    device_id=dev(there),
                    device_id_type=MESH,
                )
            )
        for c in copies[::-1]:
            c.start()

        def finish():
            for k in range(1, chips):
                there = at(k)
                pltpu.make_async_remote_copy(
                    src_ref=send.at[there],
                    dst_ref=recv.at[there],
                    send_sem=swap_send.at[n, 0],
                    recv_sem=swap_recv.at[n, there],
                    device_id=dev(there),
                    device_id_type=MESH,
                ).wait_recv()
            for c in copies:
                c.wait_send()

        return finish

    def sum_at_owner(n):
        started = []

        def copy(edge, block, where):
            k = SLOT[edge]
            return pltpu.make_async_remote_copy(
                src_ref=part_send.at[n, block],
                dst_ref=part_recv.at[n, k],
                send_sem=sum_send.at[n, k],
                recv_sem=sum_recv.at[n, k],
                device_id=dev(where),
                device_id_type=MESH,
            )

        def gathered(sign, f):
            total = part32[at(-sign * f)]
            for edge in EDGES[::-1]:
                if edge[0] == sign and edge[1] == f:
                    copy(edge, chip, chip).wait_recv()
                    total = total + part_recv[n, SLOT[edge]].astype(F32)
            return total

        inner = {(sign, f) for sign, f, _ in EDGES}
        leaves = [e for e in EDGES if (e[0], e[2]) not in inner]
        order = sorted(leaves, key=lambda e: -e[2])
        order += [(s, f, t) for s, f, t in EDGES[::-1] if (s, t) in inner]
        for sign, f, t in order:
            block = at(-sign * t)
            if (sign, t) in inner:
                part_send[n, block] = gathered(sign, t).astype(BF16)
            c = copy((sign, f, t), block, at(-sign * (t - f)))
            c.start()
            started.append(c)
        total = part32[chip]
        for sign in (1, -1):
            for edge in EDGES[::-1]:
                if edge[0] == sign and edge[1] == 0:
                    copy(edge, chip, chip).wait_recv()
                    total = total + part_recv[n, SLOT[edge]].astype(F32)
        return total, started

    gather = all_gather(rows_a, 0)
    next(gather)
    for k in (0, 1, 2, 3):
        pair[k].start()
    local[8].start()
    for k in (4, 5, 6, 7):
        local[k].start()
        pair[k].start()

    old = conv_state_ref[...]
    taps = conv_weight_ref[...].astype(F32)
    new_conv_ref[0] = old[1]
    new_conv_ref[1] = old[2]
    conv_part[...] = (
        old[0].astype(F32) * taps[0:1] + old[1].astype(F32) * taps[1:2] + old[2].astype(F32) * taps[2:3]
    )
    step_raw = nt_dot(normed, step_weight_ref[...]) + step_bias_ref[...]
    step = jnp.maximum(step_raw, 0.0) + jnp.log1p(jnp.exp(-jnp.abs(step_raw)))
    rate = jnp.exp(-step * jnp.exp(decay_log_ref[...]))
    rate_ref[...] = rate
    spread = (
        lax.broadcasted_iota(jnp.int32, (heads, width), 1) // head_dim == lax.broadcasted_iota(jnp.int32, (heads, width), 0)
    ).astype(F32)
    wide = jnp.concatenate([step, rate, jnp.broadcast_to(skip_gain_ref[...], step.shape)], axis=0)
    reps[...] = jnp.dot(wide, spread, precision=lax.Precision.HIGHEST, preferred_element_type=F32)
    eye = (
        lax.broadcasted_iota(jnp.int32, (seqs, seqs), 0) == lax.broadcasted_iota(jnp.int32, (seqs, seqs), 1)
    ).astype(F32)

    def turned(values):
        return lax.dot_general(
            eye, values, (((1,), (1,)), ((), ())), precision=lax.Precision.HIGHEST, preferred_element_type=F32
        )

    ids = turned(ids_ref[...].astype(F32))
    route = turned(route_ref[...])
    shared = chips // EXPERTS
    proj_w[4 * half + 4 * thin :] = jnp.zeros((proj_w.shape[0] - 4 * half - 4 * thin, width), BF16)

    for _ in gather:
        pass
    for k in (0, 1, 2, 3):
        local[k].wait()
        pair[k].wait()

    proj = nt_dot(rows_a[...].reshape(chips * seqs, width), proj_w[...])
    lane = lax.broadcasted_iota(jnp.int32, (seqs, 128), 1)
    for j in range(chips):
        block = proj[j * seqs : (j + 1) * seqs]
        mine = jnp.where(ids == (j // shared), route, 0.0)
        mine = jnp.sum(mine, axis=1, keepdims=True)
        high = mine.astype(BF16).astype(F32)
        tail = jnp.where(
            lane == 64, high, jnp.where(lane == 65, mine - high, block[:, 4 * half :])
        )
        proj_send[j, :, : 4 * half] = block[:, : 4 * half].astype(BF16)
        proj_send[j, :, 4 * half :] = tail.astype(BF16)
    proj_recv[chip] = proj_send[chip]
    swap(proj_send, proj_recv, 0)()

    maps = []
    for first in (0, 2 * thin):
        for g in range(groups):
            total = jnp.zeros((seqs, 128), F32)
            for i in range(4):
                piece = proj_recv[4 * g + i, :, 4 * half :].astype(F32)
                shift = (2 * thin * i - first) % 128
                if shift:
                    piece = pltpu.roll(piece, shift, 1)
                total = jnp.where((lane >= 2 * thin * i) & (lane < 2 * thin * (i + 1)), piece, total)
            maps.append(total)
    gate = jnp.concatenate([proj_recv[j, :, :lanes] for j in range(chips)], axis=1).astype(F32)
    new_row = jnp.concatenate(
        [proj_recv[j, :, lanes : 2 * lanes].astype(F32) for j in range(chips)] + maps, axis=1
    )
    new_conv_ref[2] = new_row.astype(BF16)
    conv = conv_part[...] + new_row * taps[3:4]
    conv = conv * jax.nn.sigmoid(conv)
    inputs = conv[:, :width]
    scaled = inputs * reps[:seqs]
    scaled_ref[...] = scaled
    maps_ref[...] = conv[:, width:]
    local[8].wait()

    row = lax.broadcasted_iota(jnp.int32, (seqs, 1), 0)
    gated_in = []
    for g in range(groups):
        write_map = conv[:, width + g * state_width : width + (g + 1) * state_width]
        first = width + (groups + g) * state_width
        read_map = conv[:, first : first + state_width]
        read = jnp.zeros((seqs, group_width), F32)
        for s in range(seqs):
            block = new_state_ref[s, g * per_group : (g + 1) * per_group].reshape(group_width, state_width)
            picked = jnp.where(row == s, read_map, 0.0).astype(BF16)
            read = read + nt_dot(picked, block.astype(BF16))
        cols = slice(g * group_width, (g + 1) * group_width)
        both = jnp.sum(write_map * read_map, axis=1, keepdims=True)
        read_out = reps[seqs : 2 * seqs, cols] * read + scaled[:, cols] * both + reps[2 * seqs :, cols] * inputs[:, cols]
        g_cols = gate[:, cols]
        gated_in.append(read_out * (g_cols * jax.nn.sigmoid(g_cols)))
    gated = rms_scale(jnp.concatenate(gated_in, axis=1), inner_gain_ref[...].astype(F32)).astype(BF16)
    for j in range(chips):
        head_send[j] = gated[:, j * lanes : (j + 1) * lanes]
    head_recv[chip] = head_send[chip]
    finish = swap(head_send, head_recv, 1)

    def update(s, carry):
        rates = jnp.broadcast_to(rate_ref[pl.ds(s, 1)], (state_width, heads)).T
        here = row == s
        for g in range(groups):
            x = scaled_ref[:, g * group_width : (g + 1) * group_width]
            m = jnp.where(here, maps_ref[:, g * state_width : (g + 1) * state_width], 0.0)
            xh, mh = x.astype(BF16), m.astype(BF16)
            xl, ml = (x - xh.astype(F32)).astype(BF16), (m - mh.astype(F32)).astype(BF16)
            outer = lax.dot_general(
                jnp.concatenate([xh, xh, xl], axis=0),
                jnp.concatenate([mh, ml, mh], axis=0),
                (((0,), (0,)), ((), ())),
                preferred_element_type=F32,
            ).reshape(per_group, head_dim, state_width)
            where = pl.ds(g * per_group, per_group)
            factor = rates[g * per_group : (g + 1) * per_group].reshape(per_group, 1, state_width)
            new_state_ref[s, where] = new_state_ref[s, where] * factor + outer
        return carry

    lax.fori_loop(0, seqs, update, 0)
    finish()
    local[4].wait()
    pair[4].wait()

    heads_here = head_recv[...].reshape(chips * seqs, lanes)
    mixed = jnp.dot(heads_here, out_w[...], preferred_element_type=F32).reshape(chips, seqs, width)
    part32[...] = mixed
    part_send[0] = mixed.astype(BF16)
    mixed_out, sums = sum_at_owner(0)
    residual = (hidden_ref[...].astype(F32) + mixed_out).astype(BF16)
    result_ref[...] = residual
    rows_e[chip] = rms_scale(residual.astype(F32), ffn_gain_ref[...].astype(F32)).astype(BF16)
    for _ in all_gather(rows_e, 1):
        pass
    for c in sums:
        c.wait_send()
    for k in (5, 6, 7):
        local[k].wait()
        pair[k].wait()

    tile = 256

    def unit_tile(i, carry):
        cols = pl.ds(pl.multiple_of(i * tile, tile), tile)
        tokens = rows_e[...].reshape(chips * seqs, width)
        g = jnp.dot(tokens, gate_w[:, cols], preferred_element_type=F32)
        u = jnp.dot(tokens, up_w[:, cols], preferred_element_type=F32)
        units[:, cols] = (g * jax.nn.sigmoid(g) * u).astype(BF16)
        return carry

    lax.fori_loop(0, units.shape[1] // tile, unit_tile, 0)
    tails = proj_recv[:, :, 4 * half :].astype(F32)
    combine = tails[:, :, 64:65] + tails[:, :, 65:66]

    def down_tile(i, carry):
        cols = pl.ds(pl.multiple_of(i * tile, tile), tile)
        out = jnp.dot(units[...], down_w[:, cols], preferred_element_type=F32)
        out = out.reshape(chips, seqs, tile) * combine
        part32[:, :, cols] = out
        part_send[1, :, :, cols] = out.astype(BF16)
        return carry

    lax.fori_loop(0, width // tile, down_tile, 0)
    moe_sum, sums = sum_at_owner(1)
    result_ref[...] = (result_ref[...].astype(F32) + moe_sum).astype(BF16)
    for c in sums:
        c.wait_send()


def solution(mesh):
    chips = mesh.shape["ep"] // 2

    def on_device(
        hidden,
        norm_gain,
        outgate_weight,
        input_weight,
        write_weight,
        read_weight,
        step_weight,
        step_bias,
        decay_log,
        skip_gain,
        conv_weight,
        conv_state,
        mixer_state,
        inner_gain,
        out_weight,
        ffn_gain,
        expert_gate,
        expert_up,
        expert_down,
        route_ids,
        route_weights,
    ):
        seqs, width = hidden.shape
        conv_dim = conv_weight.shape[1]
        hidden_units = expert_gate.shape[1]
        half, thin = outgate_weight.shape[1], write_weight.shape[1]
        proj_cols = -(-(4 * half + 4 * thin + 2) // 128) * 128
        lanes = width // chips
        operands = (
            (hidden, 0),
            (norm_gain.reshape(1, -1), 0),
            (outgate_weight.T, 1),
            (input_weight.T, 1),
            (write_weight.T, 1),
            (read_weight.T, 1),
            (step_weight.T, 0),
            (step_bias.reshape(1, -1), 0),
            (decay_log.reshape(1, -1), 0),
            (skip_gain.reshape(1, -1), 0),
            (conv_weight, 0),
            (conv_state.transpose(1, 0, 2), 0),
            (mixer_state, 1),
            (inner_gain.reshape(1, -1), 0),
            (out_weight, 1),
            (ffn_gain.reshape(1, -1), 0),
            (expert_gate, 1),
            (expert_up, 1),
            (expert_down, 1),
            (route_ids.T, 0),
            (route_weights.T, 0),
        )
        vmem = pl.BlockSpec(memory_space=pltpu.VMEM)
        hbm = pl.BlockSpec(memory_space=pltpu.HBM)
        edges = len(EDGES)
        result, new_state, new_conv = pl.pallas_call(
            functools.partial(step_kernel, chips),
            out_shape=(
                jax.ShapeDtypeStruct((seqs, width), BF16),
                pltpu.VMEM(mixer_state.shape, F32),
                jax.ShapeDtypeStruct((conv_state.shape[1], seqs, conv_dim), BF16),
            ),
            in_specs=[hbm if big else vmem for _, big in operands],
            out_specs=(vmem, vmem, vmem),
            scratch_shapes=[
                pltpu.VMEM((chips, seqs, width), BF16),
                pltpu.VMEM((chips, seqs, width), BF16),
                pltpu.VMEM((proj_cols, width), BF16),
                pltpu.VMEM((2 * half, width), BF16),
                pltpu.VMEM((width, 2 * hidden_units), BF16),
                pltpu.VMEM((width, 2 * hidden_units), BF16),
                pltpu.VMEM((2 * hidden_units, width), BF16),
                pltpu.VMEM((chips, seqs, proj_cols), BF16),
                pltpu.VMEM((chips, seqs, proj_cols), BF16),
                pltpu.VMEM((chips, seqs, lanes), BF16),
                pltpu.VMEM((chips, seqs, lanes), BF16),
                pltpu.VMEM((chips, seqs, width), F32),
                pltpu.VMEM((2, chips, seqs, width), BF16),
                pltpu.VMEM((2, edges, seqs, width), BF16),
                pltpu.VMEM((chips * seqs, 2 * hidden_units), BF16),
                pltpu.VMEM((3 * seqs, width), F32),
                pltpu.VMEM((seqs, conv_dim), F32),
                pltpu.VMEM((seqs, width), F32),
                pltpu.VMEM((seqs, conv_dim - width), F32),
                pltpu.VMEM((seqs, step_weight.shape[1]), F32),
                pltpu.SemaphoreType.DMA((9,)),
                pltpu.SemaphoreType.DMA((8,)),
                pltpu.SemaphoreType.DMA((8,)),
                pltpu.SemaphoreType.DMA((2, edges)),
                pltpu.SemaphoreType.DMA((2, edges)),
                pltpu.SemaphoreType.DMA((2, chips)),
                pltpu.SemaphoreType.DMA((2, chips)),
                pltpu.SemaphoreType.DMA((2, edges)),
                pltpu.SemaphoreType.DMA((2, edges)),
            ],
            compiler_params=pltpu.CompilerParams(
                collective_id=0, has_side_effects=True, vmem_limit_bytes=54 * 2**20
            ),
            name="step",
        )(*[value for value, _ in operands])
        return result, new_state, new_conv.transpose(1, 0, 2)

    return jax.shard_map(
        on_device,
        mesh=mesh,
        in_specs=(
            P(GRP_EP, None),
            P(),
            P(None, "ep"),
            P(None, "ep"),
            P(None, "ep"),
            P(None, "ep"),
            P(),
            P(),
            P(),
            P(),
            P(),
            P(GRP_EP, None, None),
            P(GRP_EP, None, None, None),
            P(),
            P("ep", None),
            P(),
            P(None, "ep"),
            P(None, "ep"),
            P("ep", None),
            P(GRP_EP, None),
            P(GRP_EP, None),
        ),
        out_specs=(P(GRP_EP, None), P(GRP_EP, None, None, None), P(GRP_EP, None, None)),
        check_vma=False,
    )
```

```python
import functools

import jax
import jax.numpy as jnp
from jax import lax
from jax.experimental import pallas as pl
from jax.experimental.pallas import tpu as pltpu
from jax.sharding import PartitionSpec as P

EXPERTS = 8
GRP_EP = ("grp", "ep")
MESH = pl.DeviceIdType.MESH
F32 = jnp.float32
BF16 = jnp.bfloat16
norm_eps = 1e-06

def both_ways(*edges):
    return tuple((sign, f, t) for (f, t) in edges for sign in (1, -1) if not (t == 8 and sign < 0))


A16 = both_ways((0, 5), (0, 2), (0, 1), (5, 8), (5, 7), (5, 6), (5, 4), (2, 3))
T13 = both_ways((0, 3), (0, 1), (3, 6), (3, 4), (1, 2), (6, 8), (6, 7), (4, 5))
TREES = (A16, T13)
GREET = sorted({way * abs(t - f) for tree in TREES for _, f, t in tree for way in (1, -1)})


def rms_scale(floats, gain):
    return floats * lax.rsqrt(jnp.mean(floats * floats, axis=-1, keepdims=True) + norm_eps) * gain


def row_of(vector_ref):
    return vector_ref[...].astype(F32).reshape(1, -1)


def nt_dot(a, b):
    return lax.dot_general(a, b, (((1,), (1,)), ((), ())), preferred_element_type=F32)


def step_kernel(
    chips,
    hidden_ref,
    norm_gain_ref,
    outgate_ref,
    input_ref,
    write_ref,
    read_ref,
    step_weight_ref,
    step_bias_ref,
    decay_log_ref,
    skip_gain_ref,
    conv_weight_ref,
    conv_state_ref,
    mixer_state_ref,
    inner_gain_ref,
    out_weight_ref,
    ffn_gain_ref,
    expert_gate_ref,
    expert_up_ref,
    expert_down_ref,
    ids_ref,
    route_ref,
    result_ref,
    new_state_ref,
    new_conv_ref,
    rows_a,
    rows_e,
    proj_w,
    out_w,
    gate_w,
    up_w,
    down_w,
    proj_send,
    proj_recv,
    head_send,
    head_recv,
    part32,
    part_send,
    part_recv,
    units,
    reps,
    conv_part,
    scaled_ref,
    maps_ref,
    rate_ref,
    total_ref,
    hidden_buf,
    norm_gain_buf,
    step_weight_buf,
    step_bias_buf,
    decay_log_buf,
    skip_gain_buf,
    conv_weight_buf,
    conv_state_buf,
    inner_gain_buf,
    ffn_gain_buf,
    ids_buf,
    route_buf,
    small_sem,
    weight_sem,
    pair_send,
    pair_recv,
    gather_send,
    gather_recv,
    swap_send,
    swap_recv,
    sum_send,
    sum_recv,
):
    seqs, width = hidden_ref.shape
    heads, head_dim, state_width = mixer_state_ref.shape[1:]
    groups = (conv_weight_ref.shape[1] - width) // (2 * state_width)
    per_group = heads // groups
    group_width = per_group * head_dim
    lanes = width // chips
    half = outgate_ref.shape[0]
    thin = write_ref.shape[0]
    hidden_units = expert_gate_ref.shape[1]
    ep = lax.axis_index("ep")
    chip, core = ep // 2, ep % 2

    def at(offset):
        return lax.rem(chip + offset + chips, chips)

    def dev(where):
        return {"ep": where * 2 + core}

    sibling = {"ep": chip * 2 + 1 - core}

    barrier = pltpu.get_barrier_semaphore()
    for offset in GREET:
        pl.semaphore_signal(barrier, inc=1, device_id=dev(at(offset)), device_id_type=MESH)
    pl.semaphore_signal(barrier, inc=1, device_id=sibling, device_id_type=MESH)

    smalls = (
        (hidden_ref, hidden_buf),
        (norm_gain_ref, norm_gain_buf),
        (step_weight_ref, step_weight_buf),
        (step_bias_ref, step_bias_buf),
        (decay_log_ref, decay_log_buf),
        (skip_gain_ref, skip_gain_buf),
        (conv_weight_ref, conv_weight_buf),
        (conv_state_ref, conv_state_buf),
        (inner_gain_ref, inner_gain_buf),
        (ffn_gain_ref, ffn_gain_buf),
        (ids_ref, ids_buf),
        (route_ref, route_buf),
    )
    small = [pltpu.make_async_copy(src, dst, small_sem.at[k]) for k, (src, dst) in enumerate(smalls)]
    for c in small:
        c.start()

    def own_rows(buf, first, count):
        return buf.at[pl.ds(pl.multiple_of(first + count * core, count), count)]

    def own_cols(buf):
        return buf.at[:, pl.ds(pl.multiple_of(hidden_units * core, 128), hidden_units)]

    shards = (
        (outgate_ref, own_rows(proj_w, 0, half)),
        (input_ref, own_rows(proj_w, 2 * half, half)),
        (write_ref, own_rows(proj_w, 4 * half, thin)),
        (read_ref, own_rows(proj_w, 4 * half + 2 * thin, thin)),
        (out_weight_ref, own_rows(out_w, 0, half)),
        (expert_gate_ref, own_cols(gate_w)),
        (expert_up_ref, own_cols(up_w)),
        (expert_down_ref, own_rows(down_w, 0, hidden_units)),
    )
    local = [pltpu.make_async_copy(src, dst, weight_sem.at[k]) for k, (src, dst) in enumerate(shards)]
    local.append(pltpu.make_async_copy(mixer_state_ref, new_state_ref, weight_sem.at[len(shards)]))
    for k in (0, 1, 2, 3):
        local[k].start()

    small[0].wait()
    small[1].wait()
    normed = rms_scale(hidden_buf[...].astype(F32), row_of(norm_gain_buf)).astype(BF16)
    rows_a[chip] = normed
    pl.semaphore_wait(barrier, len(GREET) + 1)

    pair = [
        pltpu.make_async_remote_copy(
            src_ref=src, dst_ref=dst, send_sem=pair_send.at[k], recv_sem=pair_recv.at[k], device_id=sibling, device_id_type=MESH
        )
        for k, (src, dst) in enumerate(shards)
    ]

    def by_core(work):
        if TREES[0] == TREES[1]:
            work(TREES[0])
        else:
            for k, tree in enumerate(TREES):
                pl.when(core == k)(functools.partial(work, tree))

    def block_copy(buf, n, tree, edge, source, where):
        k = tree.index(edge)
        return pltpu.make_async_remote_copy(
            src_ref=buf.at[source],
            dst_ref=buf.at[source],
            send_sem=gather_send.at[n, k],
            recv_sem=gather_recv.at[n, k],
            device_id=dev(where),
            device_id_type=MESH,
        )

    def gather_start(buf, n, tree):
        for sign, f, t in tree:
            if f == 0:
                block_copy(buf, n, tree, (sign, f, t), chip, at(sign * t)).start()

    def gather_finish(buf, n, tree):
        seen = set()

        def arrive(sign, offset):
            if (sign, offset) not in seen:
                seen.add((sign, offset))
                (edge,) = [e for e in tree if e[0] == sign and e[2] == offset]
                block_copy(buf, n, tree, edge, at(-sign * offset), chip).wait_recv()

        for sign, f, t in tree:
            if f:
                arrive(sign, f)
                block_copy(buf, n, tree, (sign, f, t), at(-sign * f), at(sign * (t - f))).start()
        for sign, f, t in tree:
            arrive(sign, t)
        for edge in tree:
            block_copy(buf, n, tree, edge, chip, chip).wait_send()

    def swap(send, recv, n):
        copies = []
        for k in range(1, chips):
            offset = (k + 1) // 2 * (1 if k % 2 else -1)
            there = at(offset)
            copies.append(
                pltpu.make_async_remote_copy(
                    src_ref=send.at[there],
                    dst_ref=recv.at[chip],
                    send_sem=swap_send.at[n, k],
                    recv_sem=swap_recv.at[n, chip],
                    device_id=dev(there),
                    device_id_type=MESH,
                )
            )
        for c in copies[::-1]:
            c.start()

        def finish():
            for k in range(1, chips):
                there = at(k)
                pltpu.make_async_remote_copy(
                    src_ref=send.at[there],
                    dst_ref=recv.at[there],
                    send_sem=swap_send.at[n, 0],
                    recv_sem=swap_recv.at[n, there],
                    device_id=dev(there),
                    device_id_type=MESH,
                ).wait_recv()
            for c in copies:
                c.wait_send()

        return finish

    def part_copy(n, tree, edge, block, where):
        k = tree.index(edge)
        return pltpu.make_async_remote_copy(
            src_ref=part_send.at[n, block],
            dst_ref=part_recv.at[n, k],
            send_sem=sum_send.at[n, k],
            recv_sem=sum_recv.at[n, k],
            device_id=dev(where),
            device_id_type=MESH,
        )

    def sum_at_owner(n, tree):
        def with_arrived(total, sign, f):
            for edge in tree:
                if edge[0] == sign and edge[1] == f:
                    part_copy(n, tree, edge, chip, chip).wait_recv()
                    total = total + part_recv[n, tree.index(edge)].astype(F32)
            return total

        inner = {(sign, f) for sign, f, _ in tree}
        far = [e for e in tree if (e[0], e[2]) not in inner and e[1]]
        near = [e for e in tree if (e[0], e[2]) not in inner and not e[1]]
        for sign, f, t in far + [e for e in tree[::-1] if (e[0], e[2]) in inner] + near:
            block = at(-sign * t)
            if (sign, t) in inner:
                part_send[n, block] = with_arrived(part32[block], sign, t).astype(BF16)
            part_copy(n, tree, (sign, f, t), block, at(-sign * (t - f))).start()
        total = part32[chip]
        for sign in (1, -1):
            total = with_arrived(total, sign, 0)
        total_ref[...] = total
        for edge in tree:
            part_copy(n, tree, edge, chip, chip).wait_send()

    by_core(functools.partial(gather_start, rows_a, 0))
    for k in (0, 1, 2, 3):
        pair[k].start()
    local[8].start()
    for k in (4, 5, 6, 7):
        local[k].start()
        pair[k].start()

    for c in small[2:]:
        c.wait()
    old = conv_state_buf[...]
    taps = conv_weight_buf[...].astype(F32)
    new_conv_ref[0] = old[1]
    new_conv_ref[1] = old[2]
    conv_part[...] = (
        old[0].astype(F32) * taps[0:1] + old[1].astype(F32) * taps[1:2] + old[2].astype(F32) * taps[2:3]
    )
    step_raw = nt_dot(normed, step_weight_buf[...]) + step_bias_buf[...]
    step = jnp.maximum(step_raw, 0.0) + jnp.log1p(jnp.exp(-jnp.abs(step_raw)))
    rate = jnp.exp(-step * jnp.exp(decay_log_buf[...]))
    rate_ref[...] = rate
    spread = (
        lax.broadcasted_iota(jnp.int32, (heads, width), 1) // head_dim == lax.broadcasted_iota(jnp.int32, (heads, width), 0)
    ).astype(F32)
    wide = jnp.concatenate([step, rate, jnp.broadcast_to(skip_gain_buf[...], step.shape)], axis=0)
    reps[...] = jnp.dot(wide, spread, precision=lax.Precision.HIGHEST, preferred_element_type=F32)
    eye = (
        lax.broadcasted_iota(jnp.int32, (seqs, seqs), 0) == lax.broadcasted_iota(jnp.int32, (seqs, seqs), 1)
    ).astype(F32)

    def turned(values):
        return lax.dot_general(
            eye, values, (((1,), (1,)), ((), ())), precision=lax.Precision.HIGHEST, preferred_element_type=F32
        )

    ids = turned(ids_buf[...].astype(F32))
    route = turned(route_buf[...])
    shared = chips // EXPERTS
    proj_w[4 * half + 4 * thin :] = jnp.zeros((proj_w.shape[0] - 4 * half - 4 * thin, width), BF16)

    by_core(functools.partial(gather_finish, rows_a, 0))
    for k in (0, 1, 2, 3):
        local[k].wait()
        pair[k].wait()

    proj = nt_dot(rows_a[...].reshape(chips * seqs, width), proj_w[...])
    lane = lax.broadcasted_iota(jnp.int32, (seqs, 128), 1)
    for j in range(chips):
        block = proj[j * seqs : (j + 1) * seqs]
        mine = jnp.where(ids == (j // shared), route, 0.0)
        mine = jnp.sum(mine, axis=1, keepdims=True)
        high = mine.astype(BF16).astype(F32)
        tail = jnp.where(
            lane == 64, high, jnp.where(lane == 65, mine - high, block[:, 4 * half :])
        )
        proj_send[j, :, : 4 * half] = block[:, : 4 * half].astype(BF16)
        proj_send[j, :, 4 * half :] = tail.astype(BF16)
    proj_recv[chip] = proj_send[chip]
    swap(proj_send, proj_recv, 0)()

    maps = []
    for first in (0, 2 * thin):
        for g in range(groups):
            total = jnp.zeros((seqs, 128), F32)
            for i in range(4):
                piece = proj_recv[4 * g + i, :, 4 * half :].astype(F32)
                shift = (2 * thin * i - first) % 128
                if shift:
                    piece = pltpu.roll(piece, shift, 1)
                total = jnp.where((lane >= 2 * thin * i) & (lane < 2 * thin * (i + 1)), piece, total)
            maps.append(total)
    gate = jnp.concatenate([proj_recv[j, :, :lanes] for j in range(chips)], axis=1).astype(F32)
    new_row = jnp.concatenate(
        [proj_recv[j, :, lanes : 2 * lanes].astype(F32) for j in range(chips)] + maps, axis=1
    )
    new_conv_ref[2] = new_row.astype(BF16)
    conv = conv_part[...] + new_row * taps[3:4]
    conv = conv * jax.nn.sigmoid(conv)
    inputs = conv[:, :width]
    scaled = inputs * reps[:seqs]
    scaled_ref[...] = scaled
    maps_ref[...] = conv[:, width:]
    local[8].wait()

    row = lax.broadcasted_iota(jnp.int32, (seqs, 1), 0)
    gated_in = []
    for g in range(groups):
        write_map = conv[:, width + g * state_width : width + (g + 1) * state_width]
        first = width + (groups + g) * state_width
        read_map = conv[:, first : first + state_width]
        read = jnp.zeros((seqs, group_width), F32)
        for s in range(seqs):
            block = new_state_ref[s, g * per_group : (g + 1) * per_group].reshape(group_width, state_width)
            picked = jnp.where(row == s, read_map, 0.0).astype(BF16)
            read = read + nt_dot(picked, block.astype(BF16))
        cols = slice(g * group_width, (g + 1) * group_width)
        both = jnp.sum(write_map * read_map, axis=1, keepdims=True)
        read_out = reps[seqs : 2 * seqs, cols] * read + scaled[:, cols] * both + reps[2 * seqs :, cols] * inputs[:, cols]
        g_cols = gate[:, cols]
        gated_in.append(read_out * (g_cols * jax.nn.sigmoid(g_cols)))
    gated = rms_scale(jnp.concatenate(gated_in, axis=1), row_of(inner_gain_buf)).astype(BF16)
    for j in range(chips):
        head_send[j] = gated[:, j * lanes : (j + 1) * lanes]
    head_recv[chip] = head_send[chip]
    finish = swap(head_send, head_recv, 1)

    def update(s, carry):
        rates = jnp.broadcast_to(rate_ref[pl.ds(s, 1)], (state_width, heads)).T
        here = row == s
        for g in range(groups):
            x = scaled_ref[:, g * group_width : (g + 1) * group_width]
            m = jnp.where(here, maps_ref[:, g * state_width : (g + 1) * state_width], 0.0)
            xh, mh = x.astype(BF16), m.astype(BF16)
            xl, ml = (x - xh.astype(F32)).astype(BF16), (m - mh.astype(F32)).astype(BF16)
            outer = lax.dot_general(
                jnp.concatenate([xh, xh, xl], axis=0),
                jnp.concatenate([mh, ml, mh], axis=0),
                (((0,), (0,)), ((), ())),
                preferred_element_type=F32,
            ).reshape(per_group, head_dim, state_width)
            where = pl.ds(g * per_group, per_group)
            factor = rates[g * per_group : (g + 1) * per_group].reshape(per_group, 1, state_width)
            new_state_ref[s, where] = new_state_ref[s, where] * factor + outer
        return carry

    lax.fori_loop(0, seqs, update, 0)
    finish()
    local[4].wait()
    pair[4].wait()

    heads_here = head_recv[...].reshape(chips * seqs, lanes)
    mixed = jnp.dot(heads_here, out_w[...], preferred_element_type=F32).reshape(chips, seqs, width)
    part32[...] = mixed
    part_send[0] = mixed.astype(BF16)
    by_core(functools.partial(sum_at_owner, 0))
    residual = (hidden_buf[...].astype(F32) + total_ref[...]).astype(BF16)
    result_ref[...] = residual
    rows_e[chip] = rms_scale(residual.astype(F32), row_of(ffn_gain_buf)).astype(BF16)
    by_core(functools.partial(gather_start, rows_e, 1))
    by_core(functools.partial(gather_finish, rows_e, 1))
    for k in (5, 6, 7):
        local[k].wait()
        pair[k].wait()

    tile = 256

    def unit_tile(i, carry):
        cols = pl.ds(pl.multiple_of(i * tile, tile), tile)
        tokens = rows_e[...].reshape(chips * seqs, width)
        g = jnp.dot(tokens, gate_w[:, cols], preferred_element_type=F32)
        u = jnp.dot(tokens, up_w[:, cols], preferred_element_type=F32)
        units[:, cols] = (g * jax.nn.sigmoid(g) * u).astype(BF16)
        return carry

    lax.fori_loop(0, units.shape[1] // tile, unit_tile, 0, unroll=True)
    tails = proj_recv[:, :, 4 * half :].astype(F32)
    combine = tails[:, :, 64:65] + tails[:, :, 65:66]

    def down_tile(i, carry):
        cols = pl.ds(pl.multiple_of(i * tile, tile), tile)
        out = jnp.dot(units[...], down_w[:, cols], preferred_element_type=F32)
        out = out.reshape(chips, seqs, tile) * combine
        part32[:, :, cols] = out
        part_send[1, :, :, cols] = out.astype(BF16)
        return carry

    lax.fori_loop(0, width // tile, down_tile, 0, unroll=True)
    by_core(functools.partial(sum_at_owner, 1))
    result_ref[...] = (result_ref[...].astype(F32) + total_ref[...]).astype(BF16)


def solution(mesh):
    chips = mesh.shape["ep"] // 2

    def on_device(
        hidden,
        norm_gain,
        outgate_weight,
        input_weight,
        write_weight,
        read_weight,
        step_weight,
        step_bias,
        decay_log,
        skip_gain,
        conv_weight,
        conv_state,
        mixer_state,
        inner_gain,
        out_weight,
        ffn_gain,
        expert_gate,
        expert_up,
        expert_down,
        route_ids,
        route_weights,
    ):
        seqs, width = hidden.shape
        conv_dim = conv_weight.shape[1]
        hidden_units = expert_gate.shape[1]
        half, thin = outgate_weight.shape[1], write_weight.shape[1]
        proj_cols = -(-(4 * half + 4 * thin + 2) // 128) * 128
        lanes = width // chips
        operands = (
            hidden,
            norm_gain,
            outgate_weight.T,
            input_weight.T,
            write_weight.T,
            read_weight.T,
            step_weight.T,
            step_bias.reshape(1, -1),
            decay_log.reshape(1, -1),
            skip_gain.reshape(1, -1),
            conv_weight,
            conv_state.transpose(1, 0, 2),
            mixer_state,
            inner_gain,
            out_weight,
            ffn_gain,
            expert_gate,
            expert_up,
            expert_down,
            route_ids.T,
            route_weights.T,
        )
        vmem = pl.BlockSpec(memory_space=pltpu.VMEM)
        hbm = pl.BlockSpec(memory_space=pl.ANY)
        smalls = [operands[k] for k in (0, 1, 6, 7, 8, 9, 10, 11, 13, 15, 19, 20)]
        edges = len(TREES[0])
        result, new_state, new_conv = pl.pallas_call(
            functools.partial(step_kernel, chips),
            out_shape=(
                pltpu.VMEM((seqs, width), BF16),
                pltpu.VMEM(mixer_state.shape, F32),
                pltpu.VMEM((conv_state.shape[1], seqs, conv_dim), BF16),
            ),
            in_specs=[hbm] * len(operands),
            out_specs=(vmem, vmem, vmem),
            scratch_shapes=[
                pltpu.VMEM((chips, seqs, width), BF16),
                pltpu.VMEM((chips, seqs, width), BF16),
                pltpu.VMEM((proj_cols, width), BF16),
                pltpu.VMEM((2 * half, width), BF16),
                pltpu.VMEM((width, 2 * hidden_units), BF16),
                pltpu.VMEM((width, 2 * hidden_units), BF16),
                pltpu.VMEM((2 * hidden_units, width), BF16),
                pltpu.VMEM((chips, seqs, proj_cols), BF16),
                pltpu.VMEM((chips, seqs, proj_cols), BF16),
                pltpu.VMEM((chips, seqs, lanes), BF16),
                pltpu.VMEM((chips, seqs, lanes), BF16),
                pltpu.VMEM((chips, seqs, width), F32),
                pltpu.VMEM((2, chips, seqs, width), BF16),
                pltpu.VMEM((2, edges, seqs, width), BF16),
                pltpu.VMEM((chips * seqs, 2 * hidden_units), BF16),
                pltpu.VMEM((3 * seqs, width), F32),
                pltpu.VMEM((seqs, conv_dim), F32),
                pltpu.VMEM((seqs, width), F32),
                pltpu.VMEM((seqs, conv_dim - width), F32),
                pltpu.VMEM((seqs, step_weight.shape[1]), F32),
                pltpu.VMEM((seqs, width), F32),
                *[pltpu.VMEM(value.shape, value.dtype) for value in smalls],
                pltpu.SemaphoreType.DMA((len(smalls),)),
                pltpu.SemaphoreType.DMA((9,)),
                pltpu.SemaphoreType.DMA((8,)),
                pltpu.SemaphoreType.DMA((8,)),
                pltpu.SemaphoreType.DMA((2, edges)),
                pltpu.SemaphoreType.DMA((2, edges)),
                pltpu.SemaphoreType.DMA((2, chips)),
                pltpu.SemaphoreType.DMA((2, chips)),
                pltpu.SemaphoreType.DMA((2, edges)),
                pltpu.SemaphoreType.DMA((2, edges)),
            ],
            compiler_params=pltpu.CompilerParams(
                collective_id=0, has_side_effects=True, vmem_limit_bytes=54 * 2**20
            ),
            name="step",
        )(*operands)
        return result, new_state, new_conv.transpose(1, 0, 2)

    return jax.shard_map(
        on_device,
        mesh=mesh,
        in_specs=(
            P(GRP_EP, None),
            P(),
            P(None, "ep"),
            P(None, "ep"),
            P(None, "ep"),
            P(None, "ep"),
            P(),
            P(),
            P(),
            P(),
            P(),
            P(GRP_EP, None, None),
            P(GRP_EP, None, None, None),
            P(),
            P("ep", None),
            P(),
            P(None, "ep"),
            P(None, "ep"),
            P("ep", None),
            P(GRP_EP, None),
            P(GRP_EP, None),
        ),
        out_specs=(P(GRP_EP, None), P(GRP_EP, None, None, None), P(GRP_EP, None, None)),
        check_vma=False,
    )
```

```python
import functools

import jax
import jax.numpy as jnp
from jax import lax
from jax.experimental import pallas as pl
from jax.experimental.pallas import tpu as pltpu
from jax.sharding import PartitionSpec as P

EXPERTS = 8
GRP_EP = ("grp", "ep")
MESH = pl.DeviceIdType.MESH
F32 = jnp.float32
BF16 = jnp.bfloat16
norm_eps = 1e-06

def both_ways(*edges):
    return tuple((sign, f, t) for (f, t) in edges for sign in (1, -1) if not (t == 8 and sign < 0))


A16 = both_ways((0, 5), (0, 2), (0, 1), (5, 8), (5, 7), (5, 6), (5, 4), (2, 3))
T13 = both_ways((0, 3), (0, 1), (3, 6), (3, 4), (1, 2), (6, 8), (6, 7), (4, 5))
TREES = ((A16, T13), (A16, T13), (A16, T13), (A16, T13))
GREET = sorted({way * abs(t - f) for pair in TREES for tree in pair for _, f, t in tree for way in (1, -1)})


def rms_scale(floats, gain):
    return floats * lax.rsqrt(jnp.mean(floats * floats, axis=-1, keepdims=True) + norm_eps) * gain


def row_of(vector_ref):
    return vector_ref[...].astype(F32).reshape(1, -1)


def nt_dot(a, b):
    return lax.dot_general(a, b, (((1,), (1,)), ((), ())), preferred_element_type=F32)


def step_kernel(
    chips,
    hidden_ref,
    norm_gain_ref,
    outgate_ref,
    input_ref,
    write_ref,
    read_ref,
    step_weight_ref,
    step_bias_ref,
    decay_log_ref,
    skip_gain_ref,
    conv_weight_ref,
    conv_state_ref,
    mixer_state_ref,
    inner_gain_ref,
    out_weight_ref,
    ffn_gain_ref,
    expert_gate_ref,
    expert_up_ref,
    expert_down_ref,
    ids_ref,
    route_ref,
    result_ref,
    new_state_ref,
    new_conv_ref,
    rows_a,
    rows_e,
    proj_w,
    out_w,
    gate_w,
    up_w,
    down_w,
    proj_send,
    proj_recv,
    head_send,
    head_recv,
    part32,
    part_send,
    part_recv,
    units,
    reps,
    conv_part,
    scaled_ref,
    maps_ref,
    rate_ref,
    total_ref,
    state16,
    hidden_buf,
    norm_gain_buf,
    step_weight_buf,
    step_bias_buf,
    decay_log_buf,
    skip_gain_buf,
    conv_weight_buf,
    conv_state_buf,
    inner_gain_buf,
    ffn_gain_buf,
    ids_buf,
    route_buf,
    small_sem,
    weight_sem,
    pair_send,
    pair_recv,
    gather_send,
    gather_recv,
    swap_send,
    swap_recv,
    sum_send,
    sum_recv,
):
    seqs, width = hidden_ref.shape
    heads, head_dim, state_width = mixer_state_ref.shape[1:]
    groups = (conv_weight_ref.shape[1] - width) // (2 * state_width)
    per_group = heads // groups
    group_width = per_group * head_dim
    lanes = width // chips
    half = outgate_ref.shape[0]
    thin = write_ref.shape[0]
    hidden_units = expert_gate_ref.shape[1]
    ep = lax.axis_index("ep")
    chip, core = ep // 2, ep % 2

    def at(offset):
        return lax.rem(chip + offset + chips, chips)

    def dev(where):
        return {"ep": where * 2 + core}

    sibling = {"ep": chip * 2 + 1 - core}

    barrier = pltpu.get_barrier_semaphore()
    for offset in GREET:
        pl.semaphore_signal(barrier, inc=1, device_id=dev(at(offset)), device_id_type=MESH)
    pl.semaphore_signal(barrier, inc=1, device_id=sibling, device_id_type=MESH)

    smalls = (
        (hidden_ref, hidden_buf),
        (norm_gain_ref, norm_gain_buf),
        (step_weight_ref, step_weight_buf),
        (step_bias_ref, step_bias_buf),
        (decay_log_ref, decay_log_buf),
        (skip_gain_ref, skip_gain_buf),
        (conv_weight_ref, conv_weight_buf),
        (conv_state_ref, conv_state_buf),
        (inner_gain_ref, inner_gain_buf),
        (ffn_gain_ref, ffn_gain_buf),
        (ids_ref, ids_buf),
        (route_ref, route_buf),
    )
    small = [pltpu.make_async_copy(src, dst, small_sem.at[k]) for k, (src, dst) in enumerate(smalls)]
    for c in small:
        c.start()

    def own_rows(buf, first, count):
        return buf.at[pl.ds(pl.multiple_of(first + count * core, count), count)]

    def own_cols(buf):
        return buf.at[:, pl.ds(pl.multiple_of(hidden_units * core, 128), hidden_units)]

    shards = (
        (outgate_ref, own_rows(proj_w, 0, half)),
        (input_ref, own_rows(proj_w, 2 * half, half)),
        (write_ref, own_rows(proj_w, 4 * half, thin)),
        (read_ref, own_rows(proj_w, 4 * half + 2 * thin, thin)),
        (out_weight_ref, own_rows(out_w, 0, half)),
        (expert_gate_ref, own_cols(gate_w)),
        (expert_up_ref, own_cols(up_w)),
        (expert_down_ref, own_rows(down_w, 0, hidden_units)),
    )
    local = [pltpu.make_async_copy(src, dst, weight_sem.at[k]) for k, (src, dst) in enumerate(shards)]
    local.append(pltpu.make_async_copy(mixer_state_ref, new_state_ref, weight_sem.at[len(shards)]))
    for k in (0, 1, 2, 3):
        local[k].start()

    small[0].wait()
    small[1].wait()
    normed = rms_scale(hidden_buf[...].astype(F32), row_of(norm_gain_buf)).astype(BF16)
    rows_a[chip] = normed
    pl.semaphore_wait(barrier, len(GREET) + 1)

    pair = [
        pltpu.make_async_remote_copy(
            src_ref=src, dst_ref=dst, send_sem=pair_send.at[k], recv_sem=pair_recv.at[k], device_id=sibling, device_id_type=MESH
        )
        for k, (src, dst) in enumerate(shards)
    ]

    def by_core(exchange, work):
        for k, tree in enumerate(TREES[exchange]):
            pl.when(core == k)(functools.partial(work, tree))

    def block_copy(buf, n, tree, edge, source, where):
        k = tree.index(edge)
        return pltpu.make_async_remote_copy(
            src_ref=buf.at[source],
            dst_ref=buf.at[source],
            send_sem=gather_send.at[n, k],
            recv_sem=gather_recv.at[n, k],
            device_id=dev(where),
            device_id_type=MESH,
        )

    def gather_start(buf, n, tree):
        for sign, f, t in tree:
            if f == 0:
                block_copy(buf, n, tree, (sign, f, t), chip, at(sign * t)).start()

    def gather_arrived(buf, n, tree, arrivals):
        for sign, offset in arrivals:
            (edge,) = [e for e in tree if e[0] == sign and e[2] == offset]
            block_copy(buf, n, tree, edge, at(-sign * offset), chip).wait_recv()

    def first_arrivals(tree):
        return [(s, f) for s, f, t in tree if f] + [(s, t) for s, f, t in tree if not f]

    def gather_relay(buf, n, tree):
        seen = set()
        for sign, f, t in tree:
            if f:
                if (sign, f) not in seen:
                    seen.add((sign, f))
                    gather_arrived(buf, n, tree, [(sign, f)])
                block_copy(buf, n, tree, (sign, f, t), at(-sign * f), at(sign * (t - f))).start()
        gather_arrived(buf, n, tree, [a for a in dict.fromkeys(first_arrivals(tree)) if a not in seen])

    def gather_last(buf, n, tree):
        first = first_arrivals(tree)
        gather_arrived(buf, n, tree, [(s, t) for s, f, t in tree if (s, t) not in first])

    def gather_sent(buf, n, tree):
        for edge in tree:
            block_copy(buf, n, tree, edge, chip, chip).wait_send()

    def swap_copy(send, recv, n, there):
        return pltpu.make_async_remote_copy(
            src_ref=send.at[there],
            dst_ref=recv.at[chip],
            send_sem=swap_send.at[n, there],
            recv_sem=swap_recv.at[n, chip],
            device_id=dev(there),
            device_id_type=MESH,
        )

    def swap_finish(send, recv, n):
        for k in range(1, chips):
            there = at(k)
            pltpu.make_async_remote_copy(
                src_ref=send.at[there],
                dst_ref=recv.at[there],
                send_sem=swap_send.at[n, there],
                recv_sem=swap_recv.at[n, there],
                device_id=dev(there),
                device_id_type=MESH,
            ).wait_recv()
        for k in range(1, chips):
            swap_copy(send, recv, n, at(k)).wait_send()

    def part_copy(n, tree, edge, block, where):
        k = tree.index(edge)
        return pltpu.make_async_remote_copy(
            src_ref=part_send.at[n, block],
            dst_ref=part_recv.at[n, k],
            send_sem=sum_send.at[n, k],
            recv_sem=sum_recv.at[n, k],
            device_id=dev(where),
            device_id_type=MESH,
        )

    def sum_at_owner(n, tree):
        def with_arrived(total, sign, f):
            for edge in tree:
                if edge[0] == sign and edge[1] == f:
                    part_copy(n, tree, edge, chip, chip).wait_recv()
                    total = total + part_recv[n, tree.index(edge)].astype(F32)
            return total

        inner = {(sign, f) for sign, f, _ in tree}
        far = [e for e in tree if (e[0], e[2]) not in inner and e[1]]
        near = [e for e in tree if (e[0], e[2]) not in inner and not e[1]]
        for sign, f, t in far + [e for e in tree[::-1] if (e[0], e[2]) in inner] + near:
            block = at(-sign * t)
            if (sign, t) in inner:
                part_send[n, block] = with_arrived(part32[block], sign, t).astype(BF16)
            part_copy(n, tree, (sign, f, t), block, at(-sign * (t - f))).start()
        total = part32[chip]
        for sign in (1, -1):
            total = with_arrived(total, sign, 0)
        total_ref[...] = total
        for edge in tree:
            part_copy(n, tree, edge, chip, chip).wait_send()

    by_core(0, functools.partial(gather_start, rows_a, 0))
    for k in (0, 1, 2, 3):
        pair[k].start()
    local[8].start()
    for k in (4, 5, 6, 7):
        local[k].start()
        pair[k].start()

    for c in small[2:]:
        c.wait()
    old = conv_state_buf[...]
    taps = conv_weight_buf[...].astype(F32)
    new_conv_ref[0] = old[1]
    new_conv_ref[1] = old[2]
    conv_part[...] = (
        old[0].astype(F32) * taps[0:1] + old[1].astype(F32) * taps[1:2] + old[2].astype(F32) * taps[2:3]
    )
    step_raw = nt_dot(normed, step_weight_buf[...]) + step_bias_buf[...]
    step = jnp.maximum(step_raw, 0.0) + jnp.log1p(jnp.exp(-jnp.abs(step_raw)))
    rate = jnp.exp(-step * jnp.exp(decay_log_buf[...]))
    rate_ref[...] = rate
    spread = (
        lax.broadcasted_iota(jnp.int32, (heads, width), 1) // head_dim == lax.broadcasted_iota(jnp.int32, (heads, width), 0)
    ).astype(F32)
    wide = jnp.concatenate([step, rate, jnp.broadcast_to(skip_gain_buf[...], step.shape)], axis=0)
    reps[...] = jnp.dot(wide, spread, precision=lax.Precision.HIGHEST, preferred_element_type=F32)
    eye = (
        lax.broadcasted_iota(jnp.int32, (seqs, seqs), 0) == lax.broadcasted_iota(jnp.int32, (seqs, seqs), 1)
    ).astype(F32)

    def turned(values):
        return lax.dot_general(
            eye, values, (((1,), (1,)), ((), ())), precision=lax.Precision.HIGHEST, preferred_element_type=F32
        )

    ids = turned(ids_buf[...].astype(F32))
    route = turned(route_buf[...])
    shared = chips // EXPERTS
    proj_w[4 * half + 4 * thin :] = jnp.zeros((proj_w.shape[0] - 4 * half - 4 * thin, width), BF16)

    lane = lax.broadcasted_iota(jnp.int32, (seqs, 128), 1)

    def project(offsets):
        there = [at(offset) for offset in offsets]
        rows = jnp.concatenate([rows_a[j] for j in there], axis=0)
        proj = nt_dot(rows, proj_w[...])
        for k, j in enumerate(there):
            block = proj[k * seqs : (k + 1) * seqs]
            mine = jnp.where(ids == (j // shared).astype(F32), route, 0.0)
            mine = jnp.sum(mine, axis=1, keepdims=True)
            high = mine.astype(BF16).astype(F32)
            tail = jnp.where(lane == 64, high, jnp.where(lane == 65, mine - high, block[:, 4 * half :]))
            proj_send[j, :, : 4 * half] = block[:, : 4 * half].astype(BF16)
            proj_send[j, :, 4 * half :] = tail.astype(BF16)
            if offsets[k]:
                swap_copy(proj_send, proj_recv, 0, j).start()

    def near_projections(tree):
        gather_relay(rows_a, 0, tree)
        for k in (0, 1, 2, 3):
            local[k].wait()
            pair[k].wait()
        first = dict.fromkeys(-s * o for s, o in first_arrivals(tree))
        project(sorted(first, key=lambda o: -abs(o)) + [0])

    def far_projections(tree):
        first = first_arrivals(tree)
        gather_last(rows_a, 0, tree)
        project(sorted((-s * t for s, f, t in tree if (s, t) not in first), key=lambda o: -abs(o)))
        gather_sent(rows_a, 0, tree)

    by_core(0, near_projections)
    local[8].wait()

    def narrow(s, carry):
        state16[s] = new_state_ref[s].astype(BF16)
        return carry

    lax.fori_loop(0, seqs, narrow, 0)
    by_core(0, far_projections)
    proj_recv[chip] = proj_send[chip]
    swap_finish(proj_send, proj_recv, 0)

    maps = []
    for first in (0, 2 * thin):
        for g in range(groups):
            total = jnp.zeros((seqs, 128), F32)
            for i in range(4):
                piece = proj_recv[4 * g + i, :, 4 * half :].astype(F32)
                shift = (2 * thin * i - first) % 128
                if shift:
                    piece = pltpu.roll(piece, shift, 1)
                total = jnp.where((lane >= 2 * thin * i) & (lane < 2 * thin * (i + 1)), piece, total)
            maps.append(total)
    gate = jnp.concatenate([proj_recv[j, :, :lanes] for j in range(chips)], axis=1).astype(F32)
    new_row = jnp.concatenate(
        [proj_recv[j, :, lanes : 2 * lanes].astype(F32) for j in range(chips)] + maps, axis=1
    )
    new_conv_ref[2] = new_row.astype(BF16)
    conv = conv_part[...] + new_row * taps[3:4]
    conv = conv * jax.nn.sigmoid(conv)
    inputs = conv[:, :width]
    scaled = inputs * reps[:seqs]
    scaled_ref[...] = scaled
    maps_ref[...] = conv[:, width:]

    row = lax.broadcasted_iota(jnp.int32, (seqs, 1), 0)
    gated_in = []
    for g in range(groups):
        write_map = conv[:, width + g * state_width : width + (g + 1) * state_width]
        first = width + (groups + g) * state_width
        read_map = conv[:, first : first + state_width]
        read = jnp.zeros((seqs, group_width), F32)
        for s in range(seqs):
            block = state16[s, g * per_group : (g + 1) * per_group].reshape(group_width, state_width)
            picked = jnp.where(row == s, read_map, 0.0).astype(BF16)
            read = read + nt_dot(picked, block)
        cols = slice(g * group_width, (g + 1) * group_width)
        both = jnp.sum(write_map * read_map, axis=1, keepdims=True)
        read_out = reps[seqs : 2 * seqs, cols] * read + scaled[:, cols] * both + reps[2 * seqs :, cols] * inputs[:, cols]
        g_cols = gate[:, cols]
        gated_in.append(read_out * (g_cols * jax.nn.sigmoid(g_cols)))
    gated = rms_scale(jnp.concatenate(gated_in, axis=1), row_of(inner_gain_buf)).astype(BF16)
    for j in range(chips):
        head_send[j] = gated[:, j * lanes : (j + 1) * lanes]
    head_recv[chip] = head_send[chip]
    for k in range(chips - 1, 0, -1):
        swap_copy(head_send, head_recv, 1, at((k + 1) // 2 * (1 if k % 2 else -1))).start()

    def update(s, carry):
        rates = jnp.broadcast_to(rate_ref[pl.ds(s, 1)], (state_width, heads)).T
        here = row == s
        for g in range(groups):
            x = scaled_ref[:, g * group_width : (g + 1) * group_width]
            m = jnp.where(here, maps_ref[:, g * state_width : (g + 1) * state_width], 0.0)
            xh, mh = x.astype(BF16), m.astype(BF16)
            xl, ml = (x - xh.astype(F32)).astype(BF16), (m - mh.astype(F32)).astype(BF16)
            outer = lax.dot_general(
                jnp.concatenate([xh, xh, xl], axis=0),
                jnp.concatenate([mh, ml, mh], axis=0),
                (((0,), (0,)), ((), ())),
                preferred_element_type=F32,
            ).reshape(per_group, head_dim, state_width)
            where = pl.ds(g * per_group, per_group)
            factor = rates[g * per_group : (g + 1) * per_group].reshape(per_group, 1, state_width)
            new_state_ref[s, where] = new_state_ref[s, where] * factor + outer
        return carry

    lax.fori_loop(0, seqs, update, 0)
    swap_finish(head_send, head_recv, 1)
    local[4].wait()
    pair[4].wait()

    heads_here = head_recv[...].reshape(chips * seqs, lanes)
    mixed = jnp.dot(heads_here, out_w[...], preferred_element_type=F32).reshape(chips, seqs, width)
    part32[...] = mixed
    part_send[0] = mixed.astype(BF16)
    by_core(1, functools.partial(sum_at_owner, 0))
    residual = (hidden_buf[...].astype(F32) + total_ref[...]).astype(BF16)
    result_ref[...] = residual
    rows_e[chip] = rms_scale(residual.astype(F32), row_of(ffn_gain_buf)).astype(BF16)
    by_core(2, functools.partial(gather_start, rows_e, 1))
    for part in (gather_relay, gather_last, gather_sent):
        by_core(2, functools.partial(part, rows_e, 1))
    for k in (5, 6, 7):
        local[k].wait()
        pair[k].wait()

    tile = 256

    def unit_tile(i, carry):
        cols = pl.ds(pl.multiple_of(i * tile, tile), tile)
        tokens = rows_e[...].reshape(chips * seqs, width)
        g = jnp.dot(tokens, gate_w[:, cols], preferred_element_type=F32)
        u = jnp.dot(tokens, up_w[:, cols], preferred_element_type=F32)
        units[:, cols] = (g * jax.nn.sigmoid(g) * u).astype(BF16)
        return carry

    lax.fori_loop(0, units.shape[1] // tile, unit_tile, 0, unroll=True)
    tails = proj_recv[:, :, 4 * half :].astype(F32)
    combine = tails[:, :, 64:65] + tails[:, :, 65:66]

    def down_tile(i, carry):
        cols = pl.ds(pl.multiple_of(i * tile, tile), tile)
        out = jnp.dot(units[...], down_w[:, cols], preferred_element_type=F32)
        out = out.reshape(chips, seqs, tile) * combine
        part32[:, :, cols] = out
        part_send[1, :, :, cols] = out.astype(BF16)
        return carry

    lax.fori_loop(0, width // tile, down_tile, 0, unroll=True)
    by_core(3, functools.partial(sum_at_owner, 1))
    result_ref[...] = (result_ref[...].astype(F32) + total_ref[...]).astype(BF16)


def store_kernel(result_in, state_in, conv_in, result_out, state_out, conv_out, sem):
    count = state_in.shape[0]
    copies = [pltpu.make_async_copy(state_in.at[k], state_out.at[k], sem.at[k]) for k in range(count)]
    copies.append(pltpu.make_async_copy(result_in, result_out, sem.at[count]))
    copies.append(pltpu.make_async_copy(conv_in, conv_out, sem.at[count + 1]))
    for c in copies:
        c.start()
    for c in copies:
        c.wait()


def solution(mesh):
    chips = mesh.shape["ep"] // 2

    def on_device(
        hidden,
        norm_gain,
        outgate_weight,
        input_weight,
        write_weight,
        read_weight,
        step_weight,
        step_bias,
        decay_log,
        skip_gain,
        conv_weight,
        conv_state,
        mixer_state,
        inner_gain,
        out_weight,
        ffn_gain,
        expert_gate,
        expert_up,
        expert_down,
        route_ids,
        route_weights,
    ):
        seqs, width = hidden.shape
        conv_dim = conv_weight.shape[1]
        hidden_units = expert_gate.shape[1]
        half, thin = outgate_weight.shape[1], write_weight.shape[1]
        proj_cols = -(-(4 * half + 4 * thin + 2) // 128) * 128
        lanes = width // chips
        operands = (
            hidden,
            norm_gain,
            outgate_weight.T,
            input_weight.T,
            write_weight.T,
            read_weight.T,
            step_weight.T,
            step_bias.reshape(1, -1),
            decay_log.reshape(1, -1),
            skip_gain.reshape(1, -1),
            conv_weight,
            conv_state.transpose(1, 0, 2),
            mixer_state,
            inner_gain,
            out_weight,
            ffn_gain,
            expert_gate,
            expert_up,
            expert_down,
            route_ids.T,
            route_weights.T,
        )
        vmem = pl.BlockSpec(memory_space=pltpu.VMEM)
        hbm = pl.BlockSpec(memory_space=pl.ANY)
        smalls = [operands[k] for k in (0, 1, 6, 7, 8, 9, 10, 11, 13, 15, 19, 20)]
        edges = len(TREES[0][0])
        result, new_state, new_conv = pl.pallas_call(
            functools.partial(step_kernel, chips),
            out_shape=(
                pltpu.VMEM((seqs, width), BF16),
                pltpu.VMEM(mixer_state.shape, F32),
                pltpu.VMEM((conv_state.shape[1], seqs, conv_dim), BF16),
            ),
            in_specs=[hbm] * len(operands),
            out_specs=(vmem, vmem, vmem),
            scratch_shapes=[
                pltpu.VMEM((chips, seqs, width), BF16),
                pltpu.VMEM((chips, seqs, width), BF16),
                pltpu.VMEM((proj_cols, width), BF16),
                pltpu.VMEM((2 * half, width), BF16),
                pltpu.VMEM((width, 2 * hidden_units), BF16),
                pltpu.VMEM((width, 2 * hidden_units), BF16),
                pltpu.VMEM((2 * hidden_units, width), BF16),
                pltpu.VMEM((chips, seqs, proj_cols), BF16),
                pltpu.VMEM((chips, seqs, proj_cols), BF16),
                pltpu.VMEM((chips, seqs, lanes), BF16),
                pltpu.VMEM((chips, seqs, lanes), BF16),
                pltpu.VMEM((chips, seqs, width), F32),
                pltpu.VMEM((2, chips, seqs, width), BF16),
                pltpu.VMEM((2, edges, seqs, width), BF16),
                pltpu.VMEM((chips * seqs, 2 * hidden_units), BF16),
                pltpu.VMEM((3 * seqs, width), F32),
                pltpu.VMEM((seqs, conv_dim), F32),
                pltpu.VMEM((seqs, width), F32),
                pltpu.VMEM((seqs, conv_dim - width), F32),
                pltpu.VMEM((seqs, step_weight.shape[1]), F32),
                pltpu.VMEM((seqs, width), F32),
                pltpu.VMEM(mixer_state.shape, BF16),
                *[pltpu.VMEM(value.shape, value.dtype) for value in smalls],
                pltpu.SemaphoreType.DMA((len(smalls),)),
                pltpu.SemaphoreType.DMA((9,)),
                pltpu.SemaphoreType.DMA((8,)),
                pltpu.SemaphoreType.DMA((8,)),
                pltpu.SemaphoreType.DMA((2, edges)),
                pltpu.SemaphoreType.DMA((2, edges)),
                pltpu.SemaphoreType.DMA((2, chips)),
                pltpu.SemaphoreType.DMA((2, chips)),
                pltpu.SemaphoreType.DMA((2, edges)),
                pltpu.SemaphoreType.DMA((2, edges)),
            ],
            compiler_params=pltpu.CompilerParams(
                collective_id=0, has_side_effects=True, vmem_limit_bytes=54 * 2**20
            ),
            name="step",
        )(*operands)
        outs = (result, new_state, new_conv)
        result, new_state, new_conv = pl.pallas_call(
            store_kernel,
            out_shape=tuple(jax.ShapeDtypeStruct(out.shape, out.dtype) for out in outs),
            in_specs=[vmem] * 3,
            out_specs=(hbm,) * 3,
            scratch_shapes=[pltpu.SemaphoreType.DMA((seqs + 2,))],
            compiler_params=pltpu.CompilerParams(vmem_limit_bytes=2**20),
            name="store",
        )(*outs)
        return result, new_state, new_conv.transpose(1, 0, 2)

    return jax.shard_map(
        on_device,
        mesh=mesh,
        in_specs=(
            P(GRP_EP, None),
            P(),
            P(None, "ep"),
            P(None, "ep"),
            P(None, "ep"),
            P(None, "ep"),
            P(),
            P(),
            P(),
            P(),
            P(),
            P(GRP_EP, None, None),
            P(GRP_EP, None, None, None),
            P(),
            P("ep", None),
            P(),
            P(None, "ep"),
            P(None, "ep"),
            P("ep", None),
            P(GRP_EP, None),
            P(GRP_EP, None),
        ),
        out_specs=(P(GRP_EP, None), P(GRP_EP, None, None, None), P(GRP_EP, None, None)),
        check_vma=False,
    )
```

```python
import functools

import jax
import jax.numpy as jnp
from jax import lax
from jax.experimental import pallas as pl
from jax.experimental.pallas import tpu as pltpu
from jax.sharding import PartitionSpec as P

EXPERTS = 8
GRP_EP = ("grp", "ep")
MESH = pl.DeviceIdType.MESH
F32 = jnp.float32
BF16 = jnp.bfloat16
norm_eps = 1e-06

def both_ways(far, *edges):
    return tuple((sign, f, t) for (f, t) in edges for sign in (far, -far) if not (t == 8 and sign != far))


A16 = both_ways(1, (0, 5), (0, 2), (0, 1), (5, 8), (5, 7), (5, 6), (5, 4), (2, 3))
T13 = both_ways(-1, (0, 3), (0, 1), (3, 6), (3, 4), (1, 2), (6, 8), (6, 7), (4, 5))
TREES = ((A16, T13), (A16, T13), (A16, T13), (A16, T13))
GREET = sorted({way * abs(t - f) for pair in TREES for tree in pair for _, f, t in tree for way in (1, -1)})


def rms_scale(floats, gain):
    return floats * lax.rsqrt(jnp.mean(floats * floats, axis=-1, keepdims=True) + norm_eps) * gain


def row_of(vector_ref):
    return vector_ref[...].astype(F32).reshape(1, -1)


def nt_dot(a, b):
    return lax.dot_general(a, b, (((1,), (1,)), ((), ())), preferred_element_type=F32)


def step_kernel(
    chips,
    hidden_ref,
    norm_gain_ref,
    outgate_ref,
    input_ref,
    write_ref,
    read_ref,
    step_weight_ref,
    step_bias_ref,
    decay_log_ref,
    skip_gain_ref,
    conv_weight_ref,
    conv_state_ref,
    mixer_state_ref,
    inner_gain_ref,
    out_weight_ref,
    ffn_gain_ref,
    expert_gate_ref,
    expert_up_ref,
    expert_down_ref,
    ids_ref,
    route_ref,
    result_ref,
    new_state_ref,
    new_conv_ref,
    rows_a,
    rows_e,
    proj_w,
    out_w,
    gate_w,
    up_w,
    down_w,
    proj_send,
    proj_recv,
    head_send,
    head_recv,
    part32,
    part_send,
    part_recv,
    units,
    reps,
    conv_part,
    scaled_ref,
    maps_ref,
    rate_ref,
    total_ref,
    state16,
    hidden_buf,
    norm_gain_buf,
    step_weight_buf,
    step_bias_buf,
    decay_log_buf,
    skip_gain_buf,
    conv_weight_buf,
    conv_state_buf,
    inner_gain_buf,
    ffn_gain_buf,
    ids_buf,
    route_buf,
    small_sem,
    weight_sem,
    pair_send,
    pair_recv,
    gather_send,
    gather_recv,
    swap_send,
    swap_recv,
    sum_send,
    sum_recv,
):
    seqs, width = hidden_ref.shape
    heads, head_dim, state_width = mixer_state_ref.shape[1:]
    groups = (conv_weight_ref.shape[1] - width) // (2 * state_width)
    per_group = heads // groups
    group_width = per_group * head_dim
    lanes = width // chips
    half = outgate_ref.shape[0]
    thin = write_ref.shape[0]
    hidden_units = expert_gate_ref.shape[1]
    ep = lax.axis_index("ep")
    chip, core = ep // 2, ep % 2

    def at(offset):
        return lax.rem(chip + offset + chips, chips)

    def dev(where):
        return {"ep": where * 2 + core}

    sibling = {"ep": chip * 2 + 1 - core}

    barrier = pltpu.get_barrier_semaphore()
    for offset in GREET:
        pl.semaphore_signal(barrier, inc=1, device_id=dev(at(offset)), device_id_type=MESH)
    pl.semaphore_signal(barrier, inc=1, device_id=sibling, device_id_type=MESH)

    smalls = (
        (hidden_ref, hidden_buf),
        (norm_gain_ref, norm_gain_buf),
        (step_weight_ref, step_weight_buf),
        (step_bias_ref, step_bias_buf),
        (decay_log_ref, decay_log_buf),
        (skip_gain_ref, skip_gain_buf),
        (conv_weight_ref, conv_weight_buf),
        (conv_state_ref, conv_state_buf),
        (inner_gain_ref, inner_gain_buf),
        (ffn_gain_ref, ffn_gain_buf),
        (ids_ref, ids_buf),
        (route_ref, route_buf),
    )
    small = [pltpu.make_async_copy(src, dst, small_sem.at[k]) for k, (src, dst) in enumerate(smalls)]
    for c in small:
        c.start()

    def own_rows(buf, first, count):
        return buf.at[pl.ds(pl.multiple_of(first + count * core, count), count)]

    def own_cols(buf):
        return buf.at[:, pl.ds(pl.multiple_of(hidden_units * core, 128), hidden_units)]

    shards = (
        (outgate_ref, own_rows(proj_w, 0, half)),
        (input_ref, own_rows(proj_w, 2 * half, half)),
        (write_ref, own_rows(proj_w, 4 * half, thin)),
        (read_ref, own_rows(proj_w, 4 * half + 2 * thin, thin)),
        (out_weight_ref, own_rows(out_w, 0, half)),
        (expert_gate_ref, own_cols(gate_w)),
        (expert_up_ref, own_cols(up_w)),
        (expert_down_ref, own_rows(down_w, 0, hidden_units)),
    )
    local = [pltpu.make_async_copy(src, dst, weight_sem.at[k]) for k, (src, dst) in enumerate(shards)]
    local.append(pltpu.make_async_copy(mixer_state_ref, new_state_ref, weight_sem.at[len(shards)]))
    for k in (0, 1, 2, 3):
        local[k].start()

    small[0].wait()
    small[1].wait()
    normed = rms_scale(hidden_buf[...].astype(F32), row_of(norm_gain_buf)).astype(BF16)
    rows_a[chip] = normed
    pl.semaphore_wait(barrier, len(GREET) + 1)

    pair = [
        pltpu.make_async_remote_copy(
            src_ref=src, dst_ref=dst, send_sem=pair_send.at[k], recv_sem=pair_recv.at[k], device_id=sibling, device_id_type=MESH
        )
        for k, (src, dst) in enumerate(shards)
    ]

    def by_core(exchange, work):
        for k, tree in enumerate(TREES[exchange]):
            pl.when(core == k)(functools.partial(work, tree))

    def block_copy(buf, n, tree, edge, source, where):
        k = tree.index(edge)
        return pltpu.make_async_remote_copy(
            src_ref=buf.at[source],
            dst_ref=buf.at[source],
            send_sem=gather_send.at[n, k],
            recv_sem=gather_recv.at[n, k],
            device_id=dev(where),
            device_id_type=MESH,
        )

    def gather_start(buf, n, tree):
        for sign, f, t in tree:
            if f == 0:
                block_copy(buf, n, tree, (sign, f, t), chip, at(sign * t)).start()

    def gather_arrived(buf, n, tree, arrivals):
        for sign, offset in arrivals:
            (edge,) = [e for e in tree if e[0] == sign and e[2] == offset]
            block_copy(buf, n, tree, edge, at(-sign * offset), chip).wait_recv()

    def first_arrivals(tree):
        return [(s, f) for s, f, t in tree if f] + [(s, t) for s, f, t in tree if not f]

    def gather_relay(buf, n, tree):
        seen = set()
        for sign, f, t in tree:
            if f:
                if (sign, f) not in seen:
                    seen.add((sign, f))
                    gather_arrived(buf, n, tree, [(sign, f)])
                block_copy(buf, n, tree, (sign, f, t), at(-sign * f), at(sign * (t - f))).start()
        gather_arrived(buf, n, tree, [a for a in dict.fromkeys(first_arrivals(tree)) if a not in seen])

    def gather_last(buf, n, tree):
        first = first_arrivals(tree)
        gather_arrived(buf, n, tree, [(s, t) for s, f, t in tree if (s, t) not in first])

    def gather_sent(buf, n, tree):
        for edge in tree:
            block_copy(buf, n, tree, edge, chip, chip).wait_send()

    def swap_copy(send, recv, n, there):
        return pltpu.make_async_remote_copy(
            src_ref=send.at[there],
            dst_ref=recv.at[chip],
            send_sem=swap_send.at[n, there],
            recv_sem=swap_recv.at[n, chip],
            device_id=dev(there),
            device_id_type=MESH,
        )

    def swap_finish(send, recv, n):
        for k in range(1, chips):
            there = at(k)
            pltpu.make_async_remote_copy(
                src_ref=send.at[there],
                dst_ref=recv.at[there],
                send_sem=swap_send.at[n, there],
                recv_sem=swap_recv.at[n, there],
                device_id=dev(there),
                device_id_type=MESH,
            ).wait_recv()
        for k in range(1, chips):
            swap_copy(send, recv, n, at(k)).wait_send()

    def part_copy(n, tree, edge, block, where):
        k = tree.index(edge)
        return pltpu.make_async_remote_copy(
            src_ref=part_send.at[n, block],
            dst_ref=part_recv.at[n, k],
            send_sem=sum_send.at[n, k],
            recv_sem=sum_recv.at[n, k],
            device_id=dev(where),
            device_id_type=MESH,
        )

    def sum_at_owner(n, tree):
        def with_arrived(total, sign, f):
            for edge in tree:
                if edge[0] == sign and edge[1] == f:
                    part_copy(n, tree, edge, chip, chip).wait_recv()
                    total = total + part_recv[n, tree.index(edge)].astype(F32)
            return total

        inner = {(sign, f) for sign, f, _ in tree}
        far = [e for e in tree if (e[0], e[2]) not in inner and e[1]]
        near = [e for e in tree if (e[0], e[2]) not in inner and not e[1]]
        for sign, f, t in far + [e for e in tree[::-1] if (e[0], e[2]) in inner] + near:
            block = at(-sign * t)
            if (sign, t) in inner:
                part_send[n, block] = with_arrived(part32[block], sign, t).astype(BF16)
            part_copy(n, tree, (sign, f, t), block, at(-sign * (t - f))).start()
        total = part32[chip]
        for sign in (1, -1):
            total = with_arrived(total, sign, 0)
        total_ref[...] = total
        for edge in tree:
            part_copy(n, tree, edge, chip, chip).wait_send()

    by_core(0, functools.partial(gather_start, rows_a, 0))
    for k in (0, 1, 2, 3):
        pair[k].start()
    local[8].start()
    for k in (4, 5, 6, 7):
        local[k].start()
        pair[k].start()

    for c in small[2:]:
        c.wait()
    old = conv_state_buf[...]
    taps = conv_weight_buf[...].astype(F32)
    new_conv_ref[0] = old[1]
    new_conv_ref[1] = old[2]
    conv_part[...] = (
        old[0].astype(F32) * taps[0:1] + old[1].astype(F32) * taps[1:2] + old[2].astype(F32) * taps[2:3]
    )
    step_raw = nt_dot(normed, step_weight_buf[...]) + step_bias_buf[...]
    step = jnp.maximum(step_raw, 0.0) + jnp.log1p(jnp.exp(-jnp.abs(step_raw)))
    rate = jnp.exp(-step * jnp.exp(decay_log_buf[...]))
    rate_ref[...] = rate
    spread = (
        lax.broadcasted_iota(jnp.int32, (heads, width), 1) // head_dim == lax.broadcasted_iota(jnp.int32, (heads, width), 0)
    ).astype(F32)
    wide = jnp.concatenate([step, rate, jnp.broadcast_to(skip_gain_buf[...], step.shape)], axis=0)
    reps[...] = jnp.dot(wide, spread, precision=lax.Precision.HIGHEST, preferred_element_type=F32)
    eye = (
        lax.broadcasted_iota(jnp.int32, (seqs, seqs), 0) == lax.broadcasted_iota(jnp.int32, (seqs, seqs), 1)
    ).astype(F32)

    def turned(values):
        return lax.dot_general(
            eye, values, (((1,), (1,)), ((), ())), precision=lax.Precision.HIGHEST, preferred_element_type=F32
        )

    ids = turned(ids_buf[...].astype(F32))
    route = turned(route_buf[...])
    shared = chips // EXPERTS
    proj_w[4 * half + 4 * thin :] = jnp.zeros((proj_w.shape[0] - 4 * half - 4 * thin, width), BF16)

    lane = lax.broadcasted_iota(jnp.int32, (seqs, 128), 1)

    def project(offsets):
        there = [at(offset) for offset in offsets]
        rows = jnp.concatenate([rows_a[j] for j in there], axis=0)
        proj = nt_dot(rows, proj_w[...])
        for k, j in enumerate(there):
            block = proj[k * seqs : (k + 1) * seqs]
            mine = jnp.where(ids == (j // shared).astype(F32), route, 0.0)
            mine = jnp.sum(mine, axis=1, keepdims=True)
            high = mine.astype(BF16).astype(F32)
            tail = jnp.where(lane == 64, high, jnp.where(lane == 65, mine - high, block[:, 4 * half :]))
            proj_send[j, :, : 4 * half] = block[:, : 4 * half].astype(BF16)
            proj_send[j, :, 4 * half :] = tail.astype(BF16)
            if offsets[k]:
                swap_copy(proj_send, proj_recv, 0, j).start()

    def near_projections(tree):
        gather_relay(rows_a, 0, tree)
        for k in (0, 1, 2, 3):
            local[k].wait()
            pair[k].wait()
        first = dict.fromkeys(-s * o for s, o in first_arrivals(tree))
        project(sorted(first, key=lambda o: -abs(o)) + [0])

    def far_projections(tree):
        first = first_arrivals(tree)
        gather_last(rows_a, 0, tree)
        project(sorted((-s * t for s, f, t in tree if (s, t) not in first), key=lambda o: -abs(o)))
        gather_sent(rows_a, 0, tree)

    by_core(0, near_projections)
    local[8].wait()

    def narrow(s, carry):
        state16[s] = new_state_ref[s].astype(BF16)
        return carry

    lax.fori_loop(0, seqs, narrow, 0)
    by_core(0, far_projections)
    proj_recv[chip] = proj_send[chip]
    swap_finish(proj_send, proj_recv, 0)

    maps = []
    for first in (0, 2 * thin):
        for g in range(groups):
            total = jnp.zeros((seqs, 128), F32)
            for i in range(4):
                piece = proj_recv[4 * g + i, :, 4 * half :].astype(F32)
                shift = (2 * thin * i - first) % 128
                if shift:
                    piece = pltpu.roll(piece, shift, 1)
                total = jnp.where((lane >= 2 * thin * i) & (lane < 2 * thin * (i + 1)), piece, total)
            maps.append(total)
    gate = jnp.concatenate([proj_recv[j, :, :lanes] for j in range(chips)], axis=1).astype(F32)
    new_row = jnp.concatenate(
        [proj_recv[j, :, lanes : 2 * lanes].astype(F32) for j in range(chips)] + maps, axis=1
    )
    new_conv_ref[2] = new_row.astype(BF16)
    conv = conv_part[...] + new_row * taps[3:4]
    conv = conv * jax.nn.sigmoid(conv)
    inputs = conv[:, :width]
    scaled = inputs * reps[:seqs]
    scaled_ref[...] = scaled
    maps_ref[...] = conv[:, width:]

    row = lax.broadcasted_iota(jnp.int32, (seqs, 1), 0)
    gated_in = []
    for g in range(groups):
        write_map = conv[:, width + g * state_width : width + (g + 1) * state_width]
        first = width + (groups + g) * state_width
        read_map = conv[:, first : first + state_width]
        read = jnp.zeros((seqs, group_width), F32)
        for s in range(seqs):
            block = state16[s, g * per_group : (g + 1) * per_group].reshape(group_width, state_width)
            picked = jnp.where(row == s, read_map, 0.0).astype(BF16)
            read = read + nt_dot(picked, block)
        cols = slice(g * group_width, (g + 1) * group_width)
        both = jnp.sum(write_map * read_map, axis=1, keepdims=True)
        read_out = reps[seqs : 2 * seqs, cols] * read + scaled[:, cols] * both + reps[2 * seqs :, cols] * inputs[:, cols]
        g_cols = gate[:, cols]
        gated_in.append(read_out * (g_cols * jax.nn.sigmoid(g_cols)))
    gated = rms_scale(jnp.concatenate(gated_in, axis=1), row_of(inner_gain_buf)).astype(BF16)
    for j in range(chips):
        head_send[j] = gated[:, j * lanes : (j + 1) * lanes]
    head_recv[chip] = head_send[chip]
    for k in range(chips - 1, 0, -1):
        swap_copy(head_send, head_recv, 1, at((k + 1) // 2 * (1 if k % 2 else -1))).start()

    def update(s, carry):
        rates = jnp.broadcast_to(rate_ref[pl.ds(s, 1)], (state_width, heads)).T
        here = row == s
        for g in range(groups):
            x = scaled_ref[:, g * group_width : (g + 1) * group_width]
            m = jnp.where(here, maps_ref[:, g * state_width : (g + 1) * state_width], 0.0)
            xh, mh = x.astype(BF16), m.astype(BF16)
            xl, ml = (x - xh.astype(F32)).astype(BF16), (m - mh.astype(F32)).astype(BF16)
            outer = lax.dot_general(
                jnp.concatenate([xh, xh, xl], axis=0),
                jnp.concatenate([mh, ml, mh], axis=0),
                (((0,), (0,)), ((), ())),
                preferred_element_type=F32,
            ).reshape(per_group, head_dim, state_width)
            where = pl.ds(g * per_group, per_group)
            factor = rates[g * per_group : (g + 1) * per_group].reshape(per_group, 1, state_width)
            new_state_ref[s, where] = new_state_ref[s, where] * factor + outer
        return carry

    lax.fori_loop(0, seqs, update, 0)
    swap_finish(head_send, head_recv, 1)
    local[4].wait()
    pair[4].wait()

    heads_here = head_recv[...].reshape(chips * seqs, lanes)
    mixed = jnp.dot(heads_here, out_w[...], preferred_element_type=F32).reshape(chips, seqs, width)
    part32[...] = mixed
    part_send[0] = mixed.astype(BF16)
    by_core(1, functools.partial(sum_at_owner, 0))
    residual = (hidden_buf[...].astype(F32) + total_ref[...]).astype(BF16)
    result_ref[...] = residual
    rows_e[chip] = rms_scale(residual.astype(F32), row_of(ffn_gain_buf)).astype(BF16)
    by_core(2, functools.partial(gather_start, rows_e, 1))
    for part in (gather_relay, gather_last, gather_sent):
        by_core(2, functools.partial(part, rows_e, 1))
    for k in (5, 6, 7):
        local[k].wait()
        pair[k].wait()

    tile = 256

    def unit_tile(i, carry):
        cols = pl.ds(pl.multiple_of(i * tile, tile), tile)
        tokens = rows_e[...].reshape(chips * seqs, width)
        g = jnp.dot(tokens, gate_w[:, cols], preferred_element_type=F32)
        u = jnp.dot(tokens, up_w[:, cols], preferred_element_type=F32)
        units[:, cols] = (g * jax.nn.sigmoid(g) * u).astype(BF16)
        return carry

    lax.fori_loop(0, units.shape[1] // tile, unit_tile, 0, unroll=True)
    tails = proj_recv[:, :, 4 * half :].astype(F32)
    combine = tails[:, :, 64:65] + tails[:, :, 65:66]

    def down_tile(i, carry):
        cols = pl.ds(pl.multiple_of(i * tile, tile), tile)
        out = jnp.dot(units[...], down_w[:, cols], preferred_element_type=F32)
        out = out.reshape(chips, seqs, tile) * combine
        part32[:, :, cols] = out
        part_send[1, :, :, cols] = out.astype(BF16)
        return carry

    lax.fori_loop(0, width // tile, down_tile, 0, unroll=True)
    by_core(3, functools.partial(sum_at_owner, 1))
    result_ref[...] = (result_ref[...].astype(F32) + total_ref[...]).astype(BF16)


def store_kernel(result_in, state_in, conv_in, result_out, state_out, conv_out, sem):
    count = state_in.shape[0]
    copies = [pltpu.make_async_copy(state_in.at[k], state_out.at[k], sem.at[k]) for k in range(count)]
    copies.append(pltpu.make_async_copy(result_in, result_out, sem.at[count]))
    copies.append(pltpu.make_async_copy(conv_in, conv_out, sem.at[count + 1]))
    for c in copies:
        c.start()
    for c in copies:
        c.wait()


def solution(mesh):
    chips = mesh.shape["ep"] // 2

    def on_device(
        hidden,
        norm_gain,
        outgate_weight,
        input_weight,
        write_weight,
        read_weight,
        step_weight,
        step_bias,
        decay_log,
        skip_gain,
        conv_weight,
        conv_state,
        mixer_state,
        inner_gain,
        out_weight,
        ffn_gain,
        expert_gate,
        expert_up,
        expert_down,
        route_ids,
        route_weights,
    ):
        seqs, width = hidden.shape
        conv_dim = conv_weight.shape[1]
        hidden_units = expert_gate.shape[1]
        half, thin = outgate_weight.shape[1], write_weight.shape[1]
        proj_cols = -(-(4 * half + 4 * thin + 2) // 128) * 128
        lanes = width // chips
        operands = (
            hidden,
            norm_gain,
            outgate_weight.T,
            input_weight.T,
            write_weight.T,
            read_weight.T,
            step_weight.T,
            step_bias.reshape(1, -1),
            decay_log.reshape(1, -1),
            skip_gain.reshape(1, -1),
            conv_weight,
            conv_state.transpose(1, 0, 2),
            mixer_state,
            inner_gain,
            out_weight,
            ffn_gain,
            expert_gate,
            expert_up,
            expert_down,
            route_ids.T,
            route_weights.T,
        )
        vmem = pl.BlockSpec(memory_space=pltpu.VMEM)
        hbm = pl.BlockSpec(memory_space=pl.ANY)
        smalls = [operands[k] for k in (0, 1, 6, 7, 8, 9, 10, 11, 13, 15, 19, 20)]
        edges = len(TREES[0][0])
        result, new_state, new_conv = pl.pallas_call(
            functools.partial(step_kernel, chips),
            out_shape=(
                pltpu.VMEM((seqs, width), BF16),
                pltpu.VMEM(mixer_state.shape, F32),
                pltpu.VMEM((conv_state.shape[1], seqs, conv_dim), BF16),
            ),
            in_specs=[hbm] * len(operands),
            out_specs=(vmem, vmem, vmem),
            scratch_shapes=[
                pltpu.VMEM((chips, seqs, width), BF16),
                pltpu.VMEM((chips, seqs, width), BF16),
                pltpu.VMEM((proj_cols, width), BF16),
                pltpu.VMEM((2 * half, width), BF16),
                pltpu.VMEM((width, 2 * hidden_units), BF16),
                pltpu.VMEM((width, 2 * hidden_units), BF16),
                pltpu.VMEM((2 * hidden_units, width), BF16),
                pltpu.VMEM((chips, seqs, proj_cols), BF16),
                pltpu.VMEM((chips, seqs, proj_cols), BF16),
                pltpu.VMEM((chips, seqs, lanes), BF16),
                pltpu.VMEM((chips, seqs, lanes), BF16),
                pltpu.VMEM((chips, seqs, width), F32),
                pltpu.VMEM((2, chips, seqs, width), BF16),
                pltpu.VMEM((2, edges, seqs, width), BF16),
                pltpu.VMEM((chips * seqs, 2 * hidden_units), BF16),
                pltpu.VMEM((3 * seqs, width), F32),
                pltpu.VMEM((seqs, conv_dim), F32),
                pltpu.VMEM((seqs, width), F32),
                pltpu.VMEM((seqs, conv_dim - width), F32),
                pltpu.VMEM((seqs, step_weight.shape[1]), F32),
                pltpu.VMEM((seqs, width), F32),
                pltpu.VMEM(mixer_state.shape, BF16),
                *[pltpu.VMEM(value.shape, value.dtype) for value in smalls],
                pltpu.SemaphoreType.DMA((len(smalls),)),
                pltpu.SemaphoreType.DMA((9,)),
                pltpu.SemaphoreType.DMA((8,)),
                pltpu.SemaphoreType.DMA((8,)),
                pltpu.SemaphoreType.DMA((2, edges)),
                pltpu.SemaphoreType.DMA((2, edges)),
                pltpu.SemaphoreType.DMA((2, chips)),
                pltpu.SemaphoreType.DMA((2, chips)),
                pltpu.SemaphoreType.DMA((2, edges)),
                pltpu.SemaphoreType.DMA((2, edges)),
            ],
            compiler_params=pltpu.CompilerParams(
                collective_id=0, has_side_effects=True, vmem_limit_bytes=54 * 2**20
            ),
            name="step",
        )(*operands)
        outs = (result, new_state, new_conv)
        result, new_state, new_conv = pl.pallas_call(
            store_kernel,
            out_shape=tuple(jax.ShapeDtypeStruct(out.shape, out.dtype) for out in outs),
            in_specs=[vmem] * 3,
            out_specs=(hbm,) * 3,
            scratch_shapes=[pltpu.SemaphoreType.DMA((seqs + 2,))],
            compiler_params=pltpu.CompilerParams(vmem_limit_bytes=2**20),
            name="store",
        )(*outs)
        return result, new_state, new_conv.transpose(1, 0, 2)

    return jax.shard_map(
        on_device,
        mesh=mesh,
        in_specs=(
            P(GRP_EP, None),
            P(),
            P(None, "ep"),
            P(None, "ep"),
            P(None, "ep"),
            P(None, "ep"),
            P(),
            P(),
            P(),
            P(),
            P(),
            P(GRP_EP, None, None),
            P(GRP_EP, None, None, None),
            P(),
            P("ep", None),
            P(),
            P(None, "ep"),
            P(None, "ep"),
            P("ep", None),
            P(GRP_EP, None),
            P(GRP_EP, None),
        ),
        out_specs=(P(GRP_EP, None), P(GRP_EP, None, None, None), P(GRP_EP, None, None)),
        check_vma=False,
    )
```
